32 devices in a mesh: sp: 8 (over z, x), tp: 4 (over y, core).
Axes of the slice: x: 2, y: 2, z: 4, core: 2. Of those that a mesh axis runs over, the one named last changes fastest.
Arguments:
- tokens: bfloat16 [768, 1024], P(('sp', 'tp')), may hold values from -11 to 11, as said below
- doc_ids: int32 [768], P('sp'), may hold values from 0 to 1, never falling along the last dimension, each value on 1 to 576 neighbouring positions
- query_down: bfloat16 [1024, 384], P('sp'), may hold values from -0.1875 to 0.1875
- query_gain: float32 [384], replicated, may hold values from 0.1 to 1.9
- query_up: bfloat16 [384, 16, 96], P('sp', 'tp'), may hold values from -0.3125 to 0.3125
- latent_down: bfloat16 [1024, 256], P('sp'), may hold values from -0.1875 to 0.1875
- latent_gain: float32 [256], replicated, may hold values from 0.1 to 1.9
- rope_down: bfloat16 [1024, 32], P('sp'), may hold values from -0.1875 to 0.1875
- key_up: bfloat16 [256, 16, 64], P('sp', 'tp'), may hold values from -0.375 to 0.375
- value_up: bfloat16 [256, 16, 64], P('sp', 'tp'), may hold values from -0.375 to 0.375
- output_weight: bfloat16 [1024, 1024], P('tp', 'sp'), may hold values from -0.1875 to 0.1875
- output_gain: float32 [1024], replicated, may hold values from 0.1 to 1.9
Outputs:
- layer_out: bfloat16 [768, 1024], P(('sp', 'tp'))
The draws below stay inside these ranges and needn't reach their ends.
Inputs may be any that keep to these rules, and one draw needn't show every extreme that they name: Every entry of tokens lies between -11 and 11. `doc_ids`: document numbers never fall along the sequence; each document holds 1 to 576 positions.
All inputs are finite; a program needn't handle non-finite values.
Results may differ from the reference program's by a relative error of at most 0.02.
Values may be sent and summed in bfloat16 or wider, within the bound.
A program may use at most 64 MiB of HBM per device.

```python
import math
import jax
import jax.numpy as jnp
import numpy as np
from jax import lax

D = 1024
HEADS = 16
Q_RANK = 384
KV_RANK = 256
ROPE_DIM = 32
NOPE_DIM = 64
V_DIM = 64
DOCS = 2
TOK_DEV = 96
HEAD_DIM = 96
TOKENS = 768
DOC_MOST = 576


def draw_tokens(key, part):
    noise_key, shift_key = jax.random.split(key)
    base_noise = jnp.clip(jax.random.normal(noise_key, (TOKENS, D), jnp.float32), -6.0, 6.0)
    offsets = jnp.clip(jax.random.normal(shift_key, (TOKENS // TOK_DEV, D), jnp.float32), -3.0, 3.0) * 1.6
    return (base_noise + jnp.repeat(offsets, TOK_DEV, axis=0)).astype(jnp.bfloat16)


def steps_of(rng, extent, cuts, smallest, high):
    level, own = 1.0, jax.random.fold_in(rng, 6)
    for axis_at, blocks in cuts:
        steps = jnp.exp(jax.random.uniform(jax.random.fold_in(own, axis_at), (blocks,), jnp.float32, smallest / len(cuts), high / len(cuts)))
        level = level * jnp.repeat(steps, extent[axis_at] // blocks).reshape([-1 if axis == axis_at else 1 for axis in range(len(extent))])
    return level


def length_profile(count, total, limit, lean):
    loads = [(1 << 20) // math.isqrt(rank ** lean) + 1 for rank in range(2, count + 1)]
    rest, counts = total - limit - (count - 1), [1] * (count - 1)
    while rest > 0:
        candidates = [i for i in range(count - 1) if counts[i] < limit]
        mass, remaining = sum([loads[i] for i in candidates]), rest
        for i in candidates:
            extra = min(limit - counts[i], max(1, remaining * loads[i] // mass), rest)
            counts[i] = counts[i] + extra
            rest = rest - extra
    return np.array([limit] + counts)


def uneven(stream_key, count, total, reach, lean):
    if count == 2:
        one = jax.random.randint(stream_key, (), max(1, total - reach), min(reach, total - 1) + 1)
        return jnp.stack([one, total - one])
    sizes = jnp.asarray(length_profile(count, total, reach, lean), jnp.int32)
    pairs = (count - 1) // 2
    donor, receiver = sizes[1:1 + 2 * pairs:2], sizes[2:2 + 2 * pairs:2]
    slack = jnp.minimum(donor - 1, reach - receiver)
    passed = jax.random.randint(jax.random.fold_in(stream_key, 1), (pairs,), 0, 1 << 20) % (slack + 1)
    sizes = sizes.at[1:1 + 2 * pairs:2].set(donor - passed).at[2:2 + 2 * pairs:2].set(receiver + passed)
    return sizes[jax.random.permutation(jax.random.fold_in(stream_key, 2), count)]


def gaussian(key, shape, scale, reach, shards=(), kind=jnp.bfloat16):
    result = scale * jax.random.normal(key, shape, jnp.float32)
    if shards:
        result = result * steps_of(key, shape, shards, -0.22, 0.18)
    return jnp.clip(result, -reach, reach).astype(kind)


def setup_inputs(seed: int = 0) -> dict:
    splits = jax.random.split(jax.random.key(seed), 13)
    return {
        "tokens": draw_tokens(jax.random.fold_in(splits[12], 71), 0),
        "doc_ids": jnp.searchsorted(jnp.cumsum(uneven(splits[1], DOCS, TOKENS, DOC_MOST, 1)), jnp.arange(TOKENS), side="right").astype(jnp.int32),
        "query_down": gaussian(splits[2], (D, Q_RANK), D ** -0.5, 0.1875, ((0, 8),)),
        "query_gain": jnp.clip(1.0 + 0.18 * jax.random.normal(splits[3], (Q_RANK,), jnp.float32), 0.1, 1.9),
        "query_up": gaussian(splits[4], (Q_RANK, HEADS, HEAD_DIM), Q_RANK ** -0.5, 0.3125, ((0, 8), (1, 4))),
        "latent_down": gaussian(splits[5], (D, KV_RANK), D ** -0.5, 0.1875, ((0, 8),)),
        "latent_gain": jnp.clip(1.0 + 0.18 * jax.random.normal(splits[6], (KV_RANK,), jnp.float32), 0.1, 1.9),
        "rope_down": gaussian(splits[7], (D, ROPE_DIM), D ** -0.5, 0.1875, ((0, 8),)),
        "key_up": gaussian(splits[8], (KV_RANK, HEADS, NOPE_DIM), KV_RANK ** -0.5, 0.375, ((0, 8), (1, 4))),
        "value_up": gaussian(splits[9], (KV_RANK, HEADS, V_DIM), KV_RANK ** -0.5, 0.375, ((0, 8), (1, 4))),
        "output_weight": gaussian(splits[10], (HEADS * V_DIM, D), (HEADS * V_DIM) ** -0.5, 0.1875, ((0, 4), (1, 8))),
        "output_gain": jnp.clip(1.0 + 0.18 * jax.random.normal(splits[11], (D,), jnp.float32), 0.1, 1.9),
    }


ROPE_BASE = 10000.0
EPS = 1e-06

def normalize(values, gain_vec):
    return values * lax.rsqrt(lax.optimization_barrier(jnp.mean(values * values, axis=-1, keepdims=True)) + EPS) * gain_vec

def rotate(rope_part, position):
    half_width = rope_part.shape[-1] // 2
    frequency = ROPE_BASE ** (-jnp.arange(0, 2 * half_width, 2, dtype=jnp.float32) / (2 * half_width))
    angles = position.astype(jnp.float32)[:, None] * frequency[None, :]
    cosine = jnp.cos(angles)
    sine_part = jnp.sin(angles)
    if rope_part.ndim == 3:
        cosine = cosine[:, None, :]
        sine_part = sine_part[:, None, :]
    first_half = rope_part[..., :half_width]
    second_half = rope_part[..., half_width:]
    return jnp.concatenate([first_half * cosine - second_half * sine_part, first_half * sine_part + second_half * cosine], axis=-1)

def reference(tokens, doc_ids, query_down, query_gain, query_up, latent_down, latent_gain, rope_down, key_up, value_up, output_weight, output_gain):
    query_lat = normalize(jnp.dot(tokens, query_down, preferred_element_type=jnp.float32), query_gain).astype(jnp.bfloat16)
    kv_lat = normalize(jnp.dot(tokens, latent_down, preferred_element_type=jnp.float32), latent_gain).astype(jnp.bfloat16)
    position = jnp.arange(TOKENS, dtype=jnp.int32)
    rope_keys = rotate(jnp.dot(tokens, rope_down, preferred_element_type=jnp.float32), position).astype(jnp.bfloat16)
    raw_query = jnp.dot(query_lat, query_up.reshape(Q_RANK, HEADS * HEAD_DIM), preferred_element_type=jnp.float32).reshape(TOKENS, HEADS, HEAD_DIM)
    queries = jnp.concatenate([raw_query[..., :NOPE_DIM], rotate(raw_query[..., NOPE_DIM:], position)], axis=-1).astype(jnp.bfloat16)
    keys_float = jnp.dot(kv_lat, key_up.reshape(KV_RANK, HEADS * NOPE_DIM), preferred_element_type=jnp.float32).reshape(TOKENS, HEADS, NOPE_DIM)
    values_float = jnp.dot(kv_lat, value_up.reshape(KV_RANK, HEADS * V_DIM), preferred_element_type=jnp.float32).reshape(TOKENS, HEADS, V_DIM)
    rope_float = rope_keys.astype(jnp.float32)
    score_scale = HEAD_DIM ** (-0.5)

    def attend_block(block_index):
        first_row = (block_index * TOK_DEV).astype(jnp.int32)
        query_block = lax.dynamic_slice_in_dim(queries, first_row, TOK_DEV, 0).astype(jnp.float32)
        id_block = lax.dynamic_slice_in_dim(doc_ids, first_row, TOK_DEV, 0)
        scores = jnp.einsum('qhe,khe->qhk', query_block[..., :NOPE_DIM], keys_float, precision=lax.Precision.HIGHEST)
        scores = scores + jnp.einsum('qhe,ke->qhk', query_block[..., NOPE_DIM:], rope_float, precision=lax.Precision.HIGHEST)
        scores = scores * score_scale
        same_doc = id_block[:, None, None] == doc_ids[None, None, :]
        scores = jnp.where(same_doc, scores, -1e+30)
        soft_weights = jax.nn.softmax(scores, axis=-1)
        return jnp.einsum('qhk,khv->qhv', soft_weights, values_float, precision=lax.Precision.HIGHEST)
    attended = lax.map(attend_block, jnp.arange(TOKENS // TOK_DEV, dtype=jnp.int32))
    attended = attended.reshape(TOKENS, HEADS * V_DIM).astype(jnp.bfloat16)
    mixed = jnp.dot(attended, output_weight, preferred_element_type=jnp.float32)
    return normalize(mixed, output_gain).astype(jnp.bfloat16)
```

```python
import functools

import jax
import jax.numpy as jnp
import numpy as np
from jax import lax
from jax.experimental import pallas as pl
from jax.experimental.pallas import tpu as pltpu
from jax.sharding import PartitionSpec as P

ROPE_BASE = 10000.0
EPS = 1e-06
MASKED = -1e30


def folded(value, axis, dim, update, carry):
    whole = jax.tree.map(lambda part: lax.all_gather(part, axis, axis=dim, tiled=True), value)
    return update(carry, whole, jnp.int32(0))


def gathered_then(share, axis, dim, apply):
    everything = lax.all_gather(share, axis, axis=dim, tiled=True)
    return apply(everything, jnp.int32(0))


def for_sending(value):
    def short(part):
        return part.astype(jnp.bfloat16) if part.dtype == jnp.float32 else part

    return jax.tree.map(short, value)


def own_rows(term, extent, axis):
    whole = term(jnp.int32(0), extent * lax.axis_size(axis)).astype(jnp.bfloat16)
    return lax.psum_scatter(whole, axis, scatter_dimension=0, tiled=True).astype(jnp.float32)


def normalize(values, gain_vec):
    return values * lax.rsqrt(jnp.mean(values * values, axis=-1, keepdims=True) + EPS) * gain_vec


def rotate(rope_part, position):
    half_width = rope_part.shape[-1] // 2
    frequency = ROPE_BASE ** (
        -jnp.arange(0, 2 * half_width, 2, dtype=jnp.float32) / (2 * half_width)
    )
    angles = position.astype(jnp.float32)[:, None] * frequency[None, :]
    cosine = jnp.cos(angles)
    sine_part = jnp.sin(angles)
    if rope_part.ndim == 3:
        cosine = cosine[:, None, :]
        sine_part = sine_part[:, None, :]
    first_half = rope_part[..., :half_width]
    second_half = rope_part[..., half_width:]
    return jnp.concatenate(
        [
            first_half * cosine - second_half * sine_part,
            first_half * sine_part + second_half * cosine,
        ],
        axis=-1,
    )


def plain_layer(
    tokens,
    doc_ids,
    query_down,
    query_gain,
    query_up,
    latent_down,
    latent_gain,
    rope_down,
    key_up,
    value_up,
    output_weight,
    output_gain,
):
    row_count = tokens.shape[0]
    key_span = doc_ids.shape[0]
    query_width = query_down.shape[1]
    latent_width = latent_down.shape[1]
    rope_width = rope_down.shape[1]
    local_heads = query_up.shape[1]
    head_width = query_up.shape[2]
    nope_width = key_up.shape[2]
    value_width = value_up.shape[2]

    def down_term(total_now, weight_rows, first_row):
        columns = lax.dynamic_slice_in_dim(tokens, first_row, weight_rows.shape[0], 1)
        return total_now + jnp.dot(columns, weight_rows, preferred_element_type=jnp.float32)

    empty_query = jnp.zeros((row_count, query_width), jnp.float32)
    empty_latent = jnp.zeros((row_count, latent_width), jnp.float32)
    empty_rope = jnp.zeros((row_count, rope_width), jnp.float32)
    query_sum = folded(query_down, "sp", 0, down_term, empty_query)
    latent_sum = folded(latent_down, "sp", 0, down_term, empty_latent)
    rope_sum = folded(rope_down, "sp", 0, down_term, empty_rope)
    query_lat = normalize(query_sum, query_gain).astype(jnp.bfloat16)
    kv_lat = normalize(latent_sum, latent_gain).astype(jnp.bfloat16)
    own_position = lax.axis_index(("sp", "tp")) * row_count + lax.iota(jnp.int32, row_count)
    rope_keys = rotate(rope_sum, own_position).astype(jnp.bfloat16)
    query_full, key_full, value_full = (
        lax.all_gather(query_up, "sp", axis=0, tiled=True),
        lax.all_gather(key_up, "sp", axis=0, tiled=True),
        lax.all_gather(value_up, "sp", axis=0, tiled=True),
    )
    flat_width = local_heads * head_width
    query_matrix = query_full.reshape(query_width, flat_width)
    block_offset = lax.axis_index("sp") * key_span

    def project(latent_rows, first_row):
        piece_rows = latent_rows.shape[0]
        raw_query = jnp.dot(
            latent_rows[:, :query_width], query_matrix, preferred_element_type=jnp.float32
        ).reshape(piece_rows, local_heads, head_width)
        position = block_offset + first_row + lax.iota(jnp.int32, piece_rows)
        turned = jnp.concatenate(
            [raw_query[..., :nope_width], rotate(raw_query[..., nope_width:], position)], axis=-1
        )
        return jnp.concatenate(
            [
                turned.astype(jnp.bfloat16).reshape(piece_rows, flat_width),
                latent_rows[:, query_width:],
            ],
            axis=1,
        )

    packed = jnp.concatenate([query_lat, kv_lat, rope_keys], axis=1)
    gathered = gathered_then(packed, "tp", 0, project)
    queries = gathered[:, :flat_width].reshape(key_span, local_heads, head_width)
    my_ids = doc_ids.astype(jnp.bfloat16)
    key_rows = jnp.concatenate([gathered[:, flat_width:], my_ids[:, None]], axis=1)
    query_nope = queries[..., :nope_width]
    query_rope = queries[..., nope_width:]
    score_scale = head_width ** (-0.5)
    absorbed = jnp.einsum("qhe,rhe->qhr", query_nope, key_full, preferred_element_type=jnp.float32)

    def block_scores(latent_part, rope_part):
        latent_float = latent_part.astype(jnp.float32)
        scores = jnp.einsum("qhr,kr->qhk", absorbed, latent_float, precision=lax.Precision.HIGHEST)
        scores = scores + jnp.einsum(
            "qhe,ke->qhk", query_rope, rope_part, preferred_element_type=jnp.float32
        )
        return (scores * score_scale, latent_float)

    def finish(averaged):
        return jnp.einsum(
            "qhr,rhv->qhv",
            averaged,
            value_full.astype(jnp.float32),
            precision=lax.Precision.HIGHEST,
        )

    def scan_step(state_now, block_keys):
        row_peak, row_total, running = state_now
        latent_part = block_keys[:, :latent_width]
        rope_part = block_keys[:, latent_width : latent_width + rope_width]
        block_ids = block_keys[:, latent_width + rope_width]
        scores, value_part = block_scores(latent_part, rope_part)
        same_doc = my_ids[:, None, None] == block_ids[None, None, :]
        peak_new = jnp.maximum(row_peak, jnp.max(jnp.where(same_doc, scores, MASKED), axis=-1))
        soft_weights = jnp.where(same_doc, jnp.exp(scores - peak_new[..., None]), 0.0)
        factor = jnp.exp(row_peak - peak_new)
        if value_part.ndim == 3:
            contrib = jnp.einsum(
                "qhk,khv->qhv", soft_weights, value_part, precision=lax.Precision.HIGHEST
            )
        else:
            contrib = jnp.einsum(
                "qhk,kv->qhv", soft_weights, value_part, precision=lax.Precision.HIGHEST
            )
        next_state = (
            peak_new,
            row_total * factor + jnp.sum(soft_weights, axis=-1),
            running * factor[..., None] + contrib,
        )
        return (next_state, None)

    def fold_keys(state_now, key_piece, first_row):
        key_blocks = key_piece.reshape(key_piece.shape[0] // key_span, key_span, key_piece.shape[1])
        return lax.scan(scan_step, state_now, key_blocks)[0]

    start_state = (
        jnp.full((key_span, local_heads), MASKED, jnp.float32),
        jnp.zeros((key_span, local_heads), jnp.float32),
        jnp.zeros((key_span, local_heads, latent_width), jnp.float32),
    )
    row_peak, row_total, running = folded(for_sending(key_rows), "sp", 0, fold_keys, start_state)
    averaged = running / row_total[..., None]
    attended = finish(averaged).astype(jnp.bfloat16).reshape(key_span, local_heads * value_width)
    out_full = lax.all_gather(output_weight, "sp", axis=1, tiled=True)

    def out_term(first_row, row_span):
        row_block = lax.dynamic_slice_in_dim(attended, first_row, row_span, 0)
        return jnp.dot(row_block, out_full, preferred_element_type=jnp.float32)

    mixed = own_rows(out_term, row_count, "tp")
    return normalize(mixed, output_gain).astype(jnp.bfloat16)


MESH = pl.DeviceIdType.MESH
LANES = 128
PENALTY = 1e6


def nt_dot(left, right):
    return lax.dot_general(
        left, right, (((1,), (1,)), ((), ())), preferred_element_type=jnp.float32
    )


def nn_dot(left, right):
    return jnp.dot(left, right, preferred_element_type=jnp.float32)


def layer_kernel(
    sizes,
    tok,
    ids,
    down,
    query_up,
    kv_up,
    out_w,
    query_gain,
    latent_gain,
    output_gain,
    table,
    out,
    tok_all,
    down_all,
    query_all,
    kvup_all,
    out_all,
    raw_all,
    row_buf,
    row_all,
    part_buf,
    part_all,
    table_buf,
    weight_send,
    weight_recv,
    row_send,
    row_recv,
    tok_send,
    tok_recv,
    raw_send,
    raw_recv,
    part_send,
    part_recv,
    local_sem,
):
    S, T, H, N, V, R = (sizes[k] for k in ("S", "T", "H", "N", "V", "R"))
    QW, LW = sizes["QW"], sizes["LW"]
    rows = tok.shape[0]
    span = rows * T
    half = S // 2
    s = lax.axis_index("sp")
    t = lax.axis_index("tp")
    pair = s + 1 - 2 * (s % 2)

    def line(k):
        return (s + 2 * k) % S

    def mate(k):
        return (t + k) % T

    table_copy = pltpu.make_async_copy(
        table.at[:, pl.ds(pl.multiple_of(s * span, 8), span)], table_buf, local_sem.at[0]
    )
    table_copy.start()

    barrier = pltpu.get_barrier_semaphore()
    for k in range(1, half):
        pl.semaphore_signal(barrier, inc=1, device_id={"sp": line(k), "tp": t}, device_id_type=MESH)
    pl.semaphore_signal(barrier, inc=1, device_id={"sp": pair, "tp": t}, device_id_type=MESH)
    for k in range(1, T):
        pl.semaphore_signal(barrier, inc=1, device_id={"sp": s, "tp": mate(k)}, device_id_type=MESH)
    pl.semaphore_wait(barrier, half - 1 + 1 + T - 1)

    def spread(own, whole, send, recv, where):
        sent = []
        for k in range(1, half):
            copy = pltpu.make_async_remote_copy(
                src_ref=own, dst_ref=whole.at[s], send_sem=send.at[where(k - 1)],
                recv_sem=recv.at[where(k - 1)], device_id={"sp": line(k), "tp": t},
                device_id_type=MESH)
            copy.start()
            sent.append(copy)
        copy = pltpu.make_async_remote_copy(
            src_ref=own, dst_ref=whole.at[s], send_sem=send.at[where(half - 1)],
            recv_sem=recv.at[where(half - 1)], device_id={"sp": pair, "tp": t},
            device_id_type=MESH)
        copy.start()
        sent.append(copy)
        return sent

    def arrival(own, whole, send, recv, slot):
        return pltpu.make_async_remote_copy(
            src_ref=own, dst_ref=whole.at[s], send_sem=send, recv_sem=recv,
            device_id={"sp": pair, "tp": t}, device_id_type=MESH)

    def pass_on(own, whole, send, recv, where, sent, k):
        arrival(own, whole, send.at[where(k - 1)], recv.at[where(k - 1)], k).wait_recv()
        block = line(half - k)
        copy = pltpu.make_async_remote_copy(
            src_ref=whole.at[block], dst_ref=whole.at[block],
            send_sem=send.at[where(half - 1 + k)], recv_sem=recv.at[where(half - 1 + k)],
            device_id={"sp": pair, "tp": t}, device_id_type=MESH)
        copy.start()
        sent.append(copy)
        return block

    def from_pair(own, whole, send, recv, where, j):
        arrival(own, whole, send.at[where(half - 1 + j)], recv.at[where(half - 1 + j)], j).wait_recv()
        return (pair + 2 * (half - j)) % S

    def to_mates(src_of, dst, send, recv):
        sent = []
        for k in range(1, T):
            copy = pltpu.make_async_remote_copy(
                src_ref=src_of(k), dst_ref=dst, send_sem=send.at[k - 1], recv_sem=recv.at[k - 1],
                device_id={"sp": s, "tp": mate(k)}, device_id_type=MESH)
            copy.start()
            sent.append(copy)
        return sent

    tok_sent = to_mates(lambda k: tok, tok_all.at[t], tok_send, tok_recv)
    arrays = [(down, down_all), (query_up, query_all), (kv_up, kvup_all), (out_w, out_all)]
    sends = [weight_send.at[i] for i in range(4)]
    recvs = [weight_recv.at[i] for i in range(4)]
    same = lambda i: i
    weight_sent = [spread(own, whole, sends[i], recvs[i], same) for i, (own, whole) in enumerate(arrays)]
    tok_all[t] = tok[...]
    for own, whole in arrays:
        whole[s] = own[...]

    def relay(i):
        own, whole = arrays[i]
        for k in range(1, half):
            pass_on(own, whole, sends[i], recvs[i], same, weight_sent[i], k)

    def rest(i):
        own, whole = arrays[i]
        for j in range(half):
            from_pair(own, whole, sends[i], recvs[i], same, j)

    relay(0)
    for copy in tok_sent:
        copy.wait_recv()
    rest(0)
    block_tokens = tok_all[...].astype(jnp.float32).reshape(span, tok.shape[1]).astype(jnp.bfloat16)
    depth = down.shape[1]
    raw = nt_dot(block_tokens[:, :depth], down_all[0])
    for j in range(1, S):
        raw = raw + nt_dot(block_tokens[:, j * depth:(j + 1) * depth], down_all[j])
    raw_all[t] = raw.astype(jnp.bfloat16)
    raw_sent = to_mates(lambda k: raw_all.at[t], raw_all.at[t], raw_send, raw_recv)
    relay(1)
    relay(2)
    table_copy.wait()
    for copy in raw_sent:
        copy.wait_recv()
    whole_raw = jnp.concatenate([raw_all[j].astype(jnp.float32) for j in range(T)], axis=1)
    query_raw = whole_raw[:, :QW]
    rope_raw = whole_raw[:, QW:QW + LANES]
    latent_raw = whole_raw[:, QW + LANES:QW + LANES + LW]
    cosine = table_buf[0]
    sine = table_buf[1]
    lane = lax.broadcasted_iota(jnp.int32, (span, LANES), 1)
    own_id = ids[...]
    h2 = R // 2
    id_lane = lane - h2
    is_id = (lane >= h2) & (lane < LANES // 2)

    def turn(x):
        return x * cosine + pltpu.roll(x, LANES // 2, 1) * sine

    key_rope = turn(rope_raw)
    key_marks = jnp.where(is_id & (id_lane != own_id), -1.0, 0.0)
    row_buf[:, :LW] = normalize(latent_raw, latent_gain[...]).astype(jnp.bfloat16)
    row_buf[:, LW:] = jnp.where(is_id, key_marks, key_rope).astype(jnp.bfloat16)
    row_sent = spread(row_buf, row_all, row_send, row_recv, same)
    row_all[s] = row_buf[...]

    query_lat = normalize(query_raw, query_gain[...]).astype(jnp.bfloat16)
    rest(1)
    queries = nn_dot(query_lat, query_all[...].reshape(QW, query_up.shape[1]))
    nope = queries[:, :H * N].astype(jnp.bfloat16)
    rope = turn(queries[:, H * N:])
    nope_lane = lax.broadcasted_iota(jnp.int32, (span, H * N), 1)
    spread_nope = jnp.concatenate(
        [jnp.where((nope_lane >= h * N) & (nope_lane < (h + 1) * N), nope, jnp.zeros_like(nope)) for h in range(H)],
        axis=0)
    is_rope = (lane < h2) | ((lane >= LANES // 2) & (lane < LANES // 2 + h2))
    query_marks = jnp.where(is_id & (id_lane == own_id), PENALTY, 0.0)
    spread_rope = jnp.concatenate(
        [jnp.where(is_rope, rope if h == 0 else pltpu.roll(rope, LANES - h * h2, 1), query_marks).astype(jnp.bfloat16) for h in range(H)],
        axis=0)
    rest(2)
    rank_rows = kv_up.shape[0] // 2
    key_matrix = kvup_all[:, :rank_rows, :].reshape(LW, kv_up.shape[1])
    value_matrix = kvup_all[:, rank_rows:, :].reshape(LW, kv_up.shape[1])
    absorbed = nt_dot(spread_nope, key_matrix).astype(jnp.bfloat16)
    for k in range(1, half):
        pass_on(row_buf, row_all, row_send, row_recv, same, row_sent, k)
    relay(3)
    for j in range(half):
        from_pair(row_buf, row_all, row_send, row_recv, same, j)
    key_rows = row_all[...].reshape(S * span, LW + LANES)
    latent_rows = key_rows[:, :LW]
    scores = nt_dot(absorbed, latent_rows) + nt_dot(spread_rope, key_rows[:, LW:])
    scores = scores * ((N + R) ** (-0.5))
    weights = jnp.exp(scores - jnp.max(scores, axis=-1, keepdims=True))
    total = jnp.sum(weights, axis=-1, keepdims=True)
    averaged = nn_dot(weights.astype(jnp.bfloat16), latent_rows) / total
    everything = nn_dot(averaged.astype(jnp.bfloat16), value_matrix)
    value_lane = lax.broadcasted_iota(jnp.int32, (span, H * V), 1)
    attended = jnp.zeros((span, H * V), jnp.float32)
    for h in range(H):
        attended = jnp.where(
            (value_lane >= h * V) & (value_lane < (h + 1) * V), everything[h * span:(h + 1) * span], attended)
    attended = attended.astype(jnp.bfloat16)
    rest(3)
    columns = out_w.shape[1]
    for j in range(S):
        part = nn_dot(attended, out_all[j])
        for i in range(T):
            part_buf[i, :, j * columns:(j + 1) * columns] = part[i * rows:(i + 1) * rows].astype(jnp.bfloat16)
    part_sent = []
    for k in range(1, T):
        copy = pltpu.make_async_remote_copy(
            src_ref=part_buf.at[mate(k)], dst_ref=part_all.at[k - 1], send_sem=part_send.at[k - 1],
            recv_sem=part_recv.at[k - 1], device_id={"sp": s, "tp": mate(k)}, device_id_type=MESH)
        copy.start()
        part_sent.append(copy)
    mixed = part_buf[t].astype(jnp.float32)
    for k in range(1, T):
        part_sent[k - 1].wait_recv()
        mixed = mixed + part_all[k - 1].astype(jnp.float32)
    out[...] = normalize(mixed, output_gain[...]).astype(jnp.bfloat16)
    for copy in tok_sent + raw_sent + row_sent + part_sent + [c for group in weight_sent for c in group]:
        copy.wait_send()


def kernel_fits(mesh, tokens, query_down, query_up, latent_down, rope_down, key_up, value_up, output_weight):
    S, T = mesh.shape["sp"], mesh.shape["tp"]
    H, N, V, R = query_up.shape[1], key_up.shape[2], value_up.shape[2], rope_down.shape[1]
    columns = query_down.shape[1] + latent_down.shape[1] + LANES
    return (
        S % 2 == 0 and S >= 4
        and tokens.shape[0] % 8 == 0
        and query_down.shape[0] % LANES == 0
        and query_down.shape[1] % LANES == 0
        and latent_down.shape[1] % LANES == 0
        and columns % (16 * T) == 0
        and query_up.shape[0] % 16 == 0
        and key_up.shape[0] % 16 == 0
        and output_weight.shape[1] % LANES == 0
        and H * R == LANES
        and H * N % LANES == 0
        and N == V
    )


def rope_tables(positions, width, copies):
    h2 = width // 2
    frequency = ROPE_BASE ** (-np.arange(0, width, 2, dtype=np.float64) / width)
    angles = np.arange(positions, dtype=np.float64)[:, None] * frequency[None, :]
    cosine = np.tile(np.cos(angles), (1, 2 * copies))
    sine = np.tile(np.sin(angles), (1, copies))
    return np.stack([cosine, np.concatenate([-sine, sine], axis=1)]).astype(np.float32)


def on_device(mesh, tokens, doc_ids, query_down, query_gain, query_up, latent_down, latent_gain,
              rope_down, key_up, value_up, output_weight, output_gain):
    if not kernel_fits(mesh, tokens, query_down, query_up, latent_down, rope_down, key_up, value_up, output_weight):
        return plain_layer(tokens, doc_ids, query_down, query_gain, query_up, latent_down, latent_gain,
                           rope_down, key_up, value_up, output_weight, output_gain)
    S, T = mesh.shape["sp"], mesh.shape["tp"]
    H, N, V, R = query_up.shape[1], key_up.shape[2], value_up.shape[2], rope_down.shape[1]
    QW, LW = query_down.shape[1], latent_down.shape[1]
    rows, width = tokens.shape
    span = rows * T
    h2 = R // 2
    depth = query_down.shape[0]
    gap = jnp.zeros((depth, LANES // 2 - h2), jnp.bfloat16)
    packed = jnp.concatenate(
        [query_down, rope_down[:, :h2], gap, rope_down[:, h2:], gap, latent_down], axis=1)
    share = packed.shape[1] // T
    down = lax.dynamic_slice_in_dim(packed, lax.axis_index("tp") * share, share, 1).T
    q_rows = query_up.shape[0]
    query_pack = jnp.concatenate(
        [query_up[..., :N].reshape(q_rows, H * N),
         query_up[..., N:].reshape(q_rows, H, 2, h2).transpose(0, 2, 1, 3).reshape(q_rows, H * R)], axis=1)
    k_rows = key_up.shape[0]
    kv_pack = jnp.concatenate([key_up.reshape(k_rows, H * N), value_up.reshape(k_rows, H * V)], axis=0)
    table = jnp.asarray(rope_tables(S * span, R, H))
    sizes = dict(S=S, T=T, H=H, N=N, V=V, R=R, QW=QW, LW=LW)
    vmem = pl.BlockSpec(memory_space=pltpu.VMEM)
    bf16 = jnp.bfloat16
    sem = pltpu.SemaphoreType.DMA
    return pl.pallas_call(
        functools.partial(layer_kernel, sizes),
        out_shape=jax.ShapeDtypeStruct((rows, width), bf16),
        in_specs=[vmem] * 9 + [pl.BlockSpec(memory_space=pl.ANY)],
        out_specs=vmem,
        scratch_shapes=[
            pltpu.VMEM((T, rows, width), bf16),
            pltpu.VMEM((S,) + down.shape, bf16),
            pltpu.VMEM((S,) + query_pack.shape, bf16),
            pltpu.VMEM((S,) + kv_pack.shape, bf16),
            pltpu.VMEM((S,) + output_weight.shape, bf16),
            pltpu.VMEM((T, span, share), bf16),
            pltpu.VMEM((span, LW + LANES), bf16),
            pltpu.VMEM((S, span, LW + LANES), bf16),
            pltpu.VMEM((T, rows, width), bf16),
            pltpu.VMEM((T - 1, rows, width), bf16),
            pltpu.VMEM((2, span, LANES), jnp.float32),
            sem((4, S - 1)),
            sem((4, S - 1)),
            sem((S - 1,)),
            sem((S - 1,)),
            sem((T - 1,)),
            sem((T - 1,)),
            sem((T - 1,)),
            sem((T - 1,)),
            sem((T - 1,)),
            sem((T - 1,)),
            sem((1,)),
        ],
        compiler_params=pltpu.CompilerParams(
            collective_id=0, has_side_effects=True, vmem_limit_bytes=48 * 1024 * 1024),
    )(tokens, doc_ids[:, None], down, query_pack, kv_pack, output_weight,
      query_gain[None, :], latent_gain[None, :], output_gain[None, :], table)


def solution(mesh):
    in_specs = (
        P(("sp", "tp"), None),
        P("sp"),
        P("sp", None),
        P(),
        P("sp", "tp", None),
        P("sp", None),
        P(),
        P("sp", None),
        P("sp", "tp", None),
        P("sp", "tp", None),
        P("tp", "sp"),
        P(),
    )
    out_specs = P(("sp", "tp"), None)
    return jax.shard_map(
        functools.partial(on_device, mesh), mesh=mesh, in_specs=in_specs, out_specs=out_specs, check_vma=False
    )
```

```python
import functools

import jax
import jax.numpy as jnp
import numpy as np
from jax import lax
from jax.experimental import pallas as pl
from jax.experimental.pallas import tpu as pltpu
from jax.sharding import PartitionSpec as P

ROPE_BASE = 10000.0
EPS = 1e-06
MASKED = -1e30


def folded(value, axis, dim, update, carry):
    whole = jax.tree.map(lambda part: lax.all_gather(part, axis, axis=dim, tiled=True), value)
    return update(carry, whole, jnp.int32(0))


def gathered_then(share, axis, dim, apply):
    everything = lax.all_gather(share, axis, axis=dim, tiled=True)
    return apply(everything, jnp.int32(0))


def for_sending(value):
    def short(part):
        return part.astype(jnp.bfloat16) if part.dtype == jnp.float32 else part

    return jax.tree.map(short, value)


def own_rows(term, extent, axis):
    whole = term(jnp.int32(0), extent * lax.axis_size(axis)).astype(jnp.bfloat16)
    return lax.psum_scatter(whole, axis, scatter_dimension=0, tiled=True).astype(jnp.float32)


def normalize(values, gain_vec):
    return values * lax.rsqrt(jnp.mean(values * values, axis=-1, keepdims=True) + EPS) * gain_vec


def rotate(rope_part, position):
    half_width = rope_part.shape[-1] // 2
    frequency = ROPE_BASE ** (
        -jnp.arange(0, 2 * half_width, 2, dtype=jnp.float32) / (2 * half_width)
    )
    angles = position.astype(jnp.float32)[:, None] * frequency[None, :]
    cosine = jnp.cos(angles)
    sine_part = jnp.sin(angles)
    if rope_part.ndim == 3:
        cosine = cosine[:, None, :]
        sine_part = sine_part[:, None, :]
    first_half = rope_part[..., :half_width]
    second_half = rope_part[..., half_width:]
    return jnp.concatenate(
        [
            first_half * cosine - second_half * sine_part,
            first_half * sine_part + second_half * cosine,
        ],
        axis=-1,
    )


def plain_layer(
    tokens,
    doc_ids,
    query_down,
    query_gain,
    query_up,
    latent_down,
    latent_gain,
    rope_down,
    key_up,
    value_up,
    output_weight,
    output_gain,
):
    row_count = tokens.shape[0]
    key_span = doc_ids.shape[0]
    query_width = query_down.shape[1]
    latent_width = latent_down.shape[1]
    rope_width = rope_down.shape[1]
    local_heads = query_up.shape[1]
    head_width = query_up.shape[2]
    nope_width = key_up.shape[2]
    value_width = value_up.shape[2]

    def down_term(total_now, weight_rows, first_row):
        columns = lax.dynamic_slice_in_dim(tokens, first_row, weight_rows.shape[0], 1)
        return total_now + jnp.dot(columns, weight_rows, preferred_element_type=jnp.float32)

    empty_query = jnp.zeros((row_count, query_width), jnp.float32)
    empty_latent = jnp.zeros((row_count, latent_width), jnp.float32)
    empty_rope = jnp.zeros((row_count, rope_width), jnp.float32)
    query_sum = folded(query_down, "sp", 0, down_term, empty_query)
    latent_sum = folded(latent_down, "sp", 0, down_term, empty_latent)
    rope_sum = folded(rope_down, "sp", 0, down_term, empty_rope)
    query_lat = normalize(query_sum, query_gain).astype(jnp.bfloat16)
    kv_lat = normalize(latent_sum, latent_gain).astype(jnp.bfloat16)
    own_position = lax.axis_index(("sp", "tp")) * row_count + lax.iota(jnp.int32, row_count)
    rope_keys = rotate(rope_sum, own_position).astype(jnp.bfloat16)
    query_full, key_full, value_full = (
        lax.all_gather(query_up, "sp", axis=0, tiled=True),
        lax.all_gather(key_up, "sp", axis=0, tiled=True),
        lax.all_gather(value_up, "sp", axis=0, tiled=True),
    )
    flat_width = local_heads * head_width
    query_matrix = query_full.reshape(query_width, flat_width)
    block_offset = lax.axis_index("sp") * key_span

    def project(latent_rows, first_row):
        piece_rows = latent_rows.shape[0]
        raw_query = jnp.dot(
            latent_rows[:, :query_width], query_matrix, preferred_element_type=jnp.float32
        ).reshape(piece_rows, local_heads, head_width)
        position = block_offset + first_row + lax.iota(jnp.int32, piece_rows)
        turned = jnp.concatenate(
            [raw_query[..., :nope_width], rotate(raw_query[..., nope_width:], position)], axis=-1
        )
        return jnp.concatenate(
            [
                turned.astype(jnp.bfloat16).reshape(piece_rows, flat_width),
                latent_rows[:, query_width:],
            ],
            axis=1,
        )

    packed = jnp.concatenate([query_lat, kv_lat, rope_keys], axis=1)
    gathered = gathered_then(packed, "tp", 0, project)
    queries = gathered[:, :flat_width].reshape(key_span, local_heads, head_width)
    my_ids = doc_ids.astype(jnp.bfloat16)
    key_rows = jnp.concatenate([gathered[:, flat_width:], my_ids[:, None]], axis=1)
    query_nope = queries[..., :nope_width]
    query_rope = queries[..., nope_width:]
    score_scale = head_width ** (-0.5)
    absorbed = jnp.einsum("qhe,rhe->qhr", query_nope, key_full, preferred_element_type=jnp.float32)

    def block_scores(latent_part, rope_part):
        latent_float = latent_part.astype(jnp.float32)
        scores = jnp.einsum("qhr,kr->qhk", absorbed, latent_float, precision=lax.Precision.HIGHEST)
        scores = scores + jnp.einsum(
            "qhe,ke->qhk", query_rope, rope_part, preferred_element_type=jnp.float32
        )
        return (scores * score_scale, latent_float)

    def finish(averaged):
        return jnp.einsum(
            "qhr,rhv->qhv",
            averaged,
            value_full.astype(jnp.float32),
            precision=lax.Precision.HIGHEST,
        )

    def scan_step(state_now, block_keys):
        row_peak, row_total, running = state_now
        latent_part = block_keys[:, :latent_width]
        rope_part = block_keys[:, latent_width : latent_width + rope_width]
        block_ids = block_keys[:, latent_width + rope_width]
        scores, value_part = block_scores(latent_part, rope_part)
        same_doc = my_ids[:, None, None] == block_ids[None, None, :]
        peak_new = jnp.maximum(row_peak, jnp.max(jnp.where(same_doc, scores, MASKED), axis=-1))
        soft_weights = jnp.where(same_doc, jnp.exp(scores - peak_new[..., None]), 0.0)
        factor = jnp.exp(row_peak - peak_new)
        if value_part.ndim == 3:
            contrib = jnp.einsum(
                "qhk,khv->qhv", soft_weights, value_part, precision=lax.Precision.HIGHEST
            )
        else:
            contrib = jnp.einsum(
                "qhk,kv->qhv", soft_weights, value_part, precision=lax.Precision.HIGHEST
            )
        next_state = (
            peak_new,
            row_total * factor + jnp.sum(soft_weights, axis=-1),
            running * factor[..., None] + contrib,
        )
        return (next_state, None)

    def fold_keys(state_now, key_piece, first_row):
        key_blocks = key_piece.reshape(key_piece.shape[0] // key_span, key_span, key_piece.shape[1])
        return lax.scan(scan_step, state_now, key_blocks)[0]

    start_state = (
        jnp.full((key_span, local_heads), MASKED, jnp.float32),
        jnp.zeros((key_span, local_heads), jnp.float32),
        jnp.zeros((key_span, local_heads, latent_width), jnp.float32),
    )
    row_peak, row_total, running = folded(for_sending(key_rows), "sp", 0, fold_keys, start_state)
    averaged = running / row_total[..., None]
    attended = finish(averaged).astype(jnp.bfloat16).reshape(key_span, local_heads * value_width)
    out_full = lax.all_gather(output_weight, "sp", axis=1, tiled=True)

    def out_term(first_row, row_span):
        row_block = lax.dynamic_slice_in_dim(attended, first_row, row_span, 0)
        return jnp.dot(row_block, out_full, preferred_element_type=jnp.float32)

    mixed = own_rows(out_term, row_count, "tp")
    return normalize(mixed, output_gain).astype(jnp.bfloat16)


MESH = pl.DeviceIdType.MESH
LANES = 128
PENALTY = 1e6


def nt_dot(left, right):
    return lax.dot_general(
        left, right, (((1,), (1,)), ((), ())), preferred_element_type=jnp.float32
    )


def nn_dot(left, right):
    return jnp.dot(left, right, preferred_element_type=jnp.float32)


def layer_kernel(
    sizes,
    tok_in,
    ids_in,
    query_down,
    latent_down,
    rope_down,
    query_up,
    key_up,
    value_up,
    out_in,
    query_gain_in,
    latent_gain_in,
    output_gain_in,
    table,
    out,
    ids,
    query_gain,
    latent_gain,
    output_gain,
    tok,
    query_down_buf,
    latent_down_buf,
    rope_down_buf,
    query_up_buf,
    key_up_buf,
    value_up_buf,
    out_w,
    table_buf,
    pack,
    query_pack,
    kv_pack,
    tok_all,
    tok_flat,
    down_all,
    query_all,
    kvup_all,
    out_all,
    raw_all,
    row_buf,
    row_all,
    part_buf,
    part_all,
    weight_send,
    weight_recv,
    row_send,
    row_recv,
    core_send,
    core_recv,
    tok_send,
    tok_recv,
    raw_send,
    raw_recv,
    part_send,
    part_recv,
    local_sem,
):
    S, T, H, N, V, R = (sizes[k] for k in ("S", "T", "H", "N", "V", "R"))
    QW, LW = sizes["QW"], sizes["LW"]
    f32, bf16 = jnp.float32, jnp.bfloat16
    rows = tok.shape[0]
    span = rows * T
    half = S // 2
    h2 = R // 2
    depth = query_down.shape[0]
    share = down_all.shape[1]
    s = lax.axis_index("sp")
    t = lax.axis_index("tp")
    pair = s + 1 - 2 * (s % 2)
    twin = t + 1 - 2 * (t % 2)

    def line(k):
        return (s + 2 * k) % S

    def mate(k):
        return (t + k) % T

    def remote(src, dst, send, recv, sp, tp):
        return pltpu.make_async_remote_copy(
            src_ref=src, dst_ref=dst, send_sem=send, recv_sem=recv,
            device_id={"sp": sp, "tp": tp}, device_id_type=MESH)

    barrier = pltpu.get_barrier_semaphore()
    for k in range(1, half):
        pl.semaphore_signal(barrier, inc=1, device_id={"sp": line(k), "tp": t}, device_id_type=MESH)
    pl.semaphore_signal(barrier, inc=1, device_id={"sp": pair, "tp": t}, device_id_type=MESH)
    for k in range(1, T):
        pl.semaphore_signal(barrier, inc=1, device_id={"sp": s, "tp": mate(k)}, device_id_type=MESH)

    loads = [
        (query_down, query_down_buf),
        (latent_down, latent_down_buf),
        (rope_down, rope_down_buf),
        (tok_in, tok),
        (query_up, query_up_buf),
        (key_up, key_up_buf),
        (value_up, value_up_buf),
        (out_in, out_w),
        (table.at[:, pl.ds(pl.multiple_of(s * span, 8), span)], table_buf),
        (ids_in, ids),
        (query_gain_in, query_gain),
        (latent_gain_in, latent_gain),
        (output_gain_in, output_gain),
    ]
    copies = []
    for i, (src, dst) in enumerate(loads):
        copy = pltpu.make_async_copy(src, dst, local_sem.at[i])
        copy.start()
        copies.append(copy)

    for copy in copies[:3]:
        copy.wait()
    pack[:QW] = query_down_buf[...].astype(f32).T.astype(bf16)
    pack[QW + LANES:] = latent_down_buf[...].astype(f32).T.astype(bf16)
    rope_cols = rope_down_buf[...].astype(f32)
    gap = jnp.zeros((LANES // 2 - h2, depth), f32)
    pack[QW:QW + LANES] = jnp.concatenate(
        [rope_cols[:h2], gap, rope_cols[h2:R], gap], axis=0).astype(bf16)
    down = pack.at[pl.ds(pl.multiple_of(t * share, 16), share)]
    copies[3].wait()
    pl.semaphore_wait(barrier, half - 1 + 1 + T - 1)

    def spread(own, view, send, recv):
        sent = []
        for k in range(1, half):
            sent.append(remote(own, view(s), send.at[k - 1], recv.at[k - 1], line(k), t))
        sent.append(remote(own, view(s), send.at[half - 1], recv.at[half - 1], pair, t))
        for copy in sent:
            copy.start()
        return sent

    def landed(view, send, recv, slot):
        remote(view(s), view(s), send.at[slot], recv.at[slot], pair, t).wait_recv()

    def pass_on(view, send, recv, sent, k):
        landed(view, send, recv, k - 1)
        block = line(half - k)
        slot = half - 1 + k
        copy = remote(view(block), view(block), send.at[slot], recv.at[slot], pair, t)
        copy.start()
        sent.append(copy)
        return block

    def pair_block(j):
        return (pair + 2 * (half - j)) % S

    def to_mates(src_of, dst, send, recv):
        sent = [remote(src_of(k), dst, send.at[k - 1], recv.at[k - 1], s, mate(k)) for k in range(1, T)]
        for copy in sent:
            copy.start()
        return sent

    wholes = [down_all, query_all, kvup_all, out_all]
    owns = [down, query_pack, kv_pack, out_w]
    views = [lambda i, w=w: w.at[i] for w in wholes]
    weight_sent = [[], [], [], []]

    def begin(i):
        weight_sent[i] += spread(owns[i], views[i], weight_send.at[i], weight_recv.at[i])

    def relay(i, then=None):
        for k in range(1, half):
            block = pass_on(views[i], weight_send.at[i], weight_recv.at[i], weight_sent[i], k)
            if then is not None:
                then(block)

    def rest(i, then=None):
        for j in range(half):
            landed(views[i], weight_send.at[i], weight_recv.at[i], half - 1 + j)
            if then is not None:
                then(pair_block(j))

    begin(0)
    tok_sent = to_mates(lambda k: tok, tok_all.at[t], tok_send, tok_recv)
    down_all[s] = down[...]
    tok_all[t] = tok[...]

    for copy in copies[4:8]:
        copy.wait()
    query_in = [query_up_buf[:, h, :].astype(f32) for h in range(H)]
    query_pack[...] = jnp.concatenate(
        [x[:, :N] for x in query_in] + [x[:, N:N + h2] for x in query_in] + [x[:, N + h2:] for x in query_in],
        axis=1).astype(bf16)
    k_rows = key_up.shape[0]
    kv_pack[:k_rows] = jnp.concatenate([key_up_buf[:, h, :].astype(f32) for h in range(H)], axis=1).astype(bf16)
    kv_pack[k_rows:] = jnp.concatenate([value_up_buf[:, h, :].astype(f32) for h in range(H)], axis=1).astype(bf16)
    query_all[s] = query_pack[...]
    kvup_all[s] = kv_pack[...]
    out_all[s] = out_w[...]

    for copy in tok_sent:
        copy.wait_recv()
    tok_flat[...] = tok_all[...].astype(f32).reshape(span, tok.shape[1]).astype(bf16)
    total_raw = [jnp.zeros((span, share), f32)]

    def down_block(block):
        columns = tok_flat[:, pl.ds(pl.multiple_of(block * depth, LANES), depth)]
        total_raw[0] = total_raw[0] + nt_dot(columns, down_all[block])

    down_block(s)
    relay(0, down_block)
    begin(1)
    begin(2)
    rest(0, down_block)
    raw_all[t] = total_raw[0].astype(bf16)
    raw_sent = to_mates(lambda k: raw_all.at[t], raw_all.at[t], raw_send, raw_recv)
    for copy in copies[8:]:
        copy.wait()
    cosine = table_buf[0]
    sine = table_buf[1]
    lane = lax.broadcasted_iota(jnp.int32, (span, LANES), 1)
    padded = -(-span // LANES) * LANES
    id_row = jnp.concatenate([ids[...].astype(f32), jnp.zeros((1, padded - span), f32)], axis=1)
    own_id = jnp.broadcast_to(id_row, (LANES, padded)).T[:span]
    id_lane = (lane - h2).astype(f32)
    is_id = (lane >= h2) & (lane < LANES // 2)

    for copy in raw_sent:
        copy.wait_recv()
    whole_raw = jnp.concatenate([raw_all[j].astype(f32) for j in range(T)], axis=1)
    query_raw = whole_raw[:, :QW]
    rope_raw = whole_raw[:, QW:QW + LANES]
    latent_raw = whole_raw[:, QW + LANES:QW + LANES + LW]

    def turn(x):
        return x * cosine + pltpu.roll(x, LANES // 2, 1) * sine

    key_marks = jnp.where(is_id & (id_lane != own_id), -1.0, 0.0)
    row_buf[:, :LW] = normalize(latent_raw, latent_gain[...]).astype(bf16)
    row_buf[:, LW:] = jnp.where(is_id, key_marks, turn(rope_raw)).astype(bf16)
    part_rows = span // 2
    mine = pl.ds(pl.multiple_of((t % 2) * part_rows, 16), part_rows)

    def row_view(i):
        return row_all.at[i, mine]

    row_sent = spread(row_buf.at[mine], row_view, row_send, row_recv)
    relay(1)
    relay(2)
    begin(3)

    query_lat = normalize(query_raw, query_gain[...]).astype(bf16)
    rest(1)
    queries = nn_dot(query_lat, query_all[...].reshape(QW, query_pack.shape[1]))
    nope = queries[:, :H * N].astype(bf16)
    rope = turn(queries[:, H * N:])
    nope_lane = lax.broadcasted_iota(jnp.int32, (span, H * N), 1)
    spread_nope = jnp.concatenate(
        [jnp.where((nope_lane >= h * N) & (nope_lane < (h + 1) * N), nope, jnp.zeros_like(nope)) for h in range(H)],
        axis=0)
    is_rope = (lane < h2) | ((lane >= LANES // 2) & (lane < LANES // 2 + h2))
    query_marks = jnp.where(is_id & (id_lane == own_id), PENALTY, 0.0)
    spread_rope = jnp.concatenate(
        [jnp.where(is_rope, rope if h == 0 else pltpu.roll(rope, LANES - h * h2, 1), query_marks).astype(bf16) for h in range(H)],
        axis=0)
    core_sent = []

    def to_twin(block, slot):
        copy = remote(row_view(block), row_view(block), core_send.at[slot], core_recv.at[slot], s, twin)
        copy.start()
        core_sent.append(copy)

    rest(2)
    key_matrix = kvup_all[:, :k_rows, :].reshape(LW, kv_pack.shape[1])
    value_matrix = kvup_all[:, k_rows:, :].reshape(LW, kv_pack.shape[1])
    absorbed = nt_dot(spread_nope, key_matrix).astype(bf16)
    wide_query = jnp.concatenate([absorbed, spread_rope], axis=1)
    scale = (N + R) ** (-0.5)

    def block_scores(key_rows):
        return nt_dot(wide_query, key_rows) * scale

    first = block_scores(row_buf[...])
    peak = jnp.max(first, axis=-1, keepdims=True)
    first = jnp.exp(first - peak)
    state = [peak, jnp.sum(first, axis=-1, keepdims=True), nn_dot(first.astype(bf16), row_buf[:, :LW])]

    def fold(blocks):
        key_rows = jnp.concatenate([row_all[b].astype(f32) for b in blocks], axis=0).astype(bf16)
        scores = block_scores(key_rows)
        peak, total, running = state
        peak_new = jnp.maximum(peak, jnp.max(scores, axis=-1, keepdims=True))
        factor = jnp.exp(peak - peak_new)
        weights = jnp.exp(scores - peak_new)
        state[0] = peak_new
        state[1] = total * factor + jnp.sum(weights, axis=-1, keepdims=True)
        state[2] = running * factor + nn_dot(weights.astype(bf16), key_rows[:, :LW])

    blocks = [pass_on(row_view, row_send, row_recv, row_sent, k) for k in range(1, half)]
    for slot, block in enumerate(blocks):
        to_twin(block, slot)
    for j in range(half):
        landed(row_view, row_send, row_recv, half - 1 + j)
        to_twin(pair_block(j), half - 1 + j)
    for copy in core_sent[:half - 1]:
        copy.wait_recv()
    fold(blocks)
    for copy in core_sent[half - 1:]:
        copy.wait_recv()
    fold([pair_block(j) for j in range(half)])
    relay(3)
    averaged = state[2] / state[1]
    everything = nn_dot(averaged.astype(bf16), value_matrix)
    value_lane = lax.broadcasted_iota(jnp.int32, (span, H * V), 1)
    attended = jnp.zeros((span, H * V), f32)
    for h in range(H):
        attended = jnp.where(
            (value_lane >= h * V) & (value_lane < (h + 1) * V), everything[h * span:(h + 1) * span], attended)
    attended = attended.astype(bf16)
    rest(3)
    columns = out_w.shape[1]
    for j in range(S):
        part = nn_dot(attended, out_all[j])
        for i in range(T):
            part_buf[i, :, j * columns:(j + 1) * columns] = part[i * rows:(i + 1) * rows].astype(bf16)
    part_sent = []
    for k in range(1, T):
        copy = remote(part_buf.at[mate(k)], part_all.at[k - 1], part_send.at[k - 1], part_recv.at[k - 1], s, mate(k))
        copy.start()
        part_sent.append(copy)
    mixed = part_buf[t].astype(f32)
    for k in range(1, T):
        part_sent[k - 1].wait_recv()
        mixed = mixed + part_all[k - 1].astype(f32)
    out[...] = normalize(mixed, output_gain[...]).astype(bf16)
    for copy in tok_sent + raw_sent + row_sent + core_sent + part_sent + [c for group in weight_sent for c in group]:
        copy.wait_send()


def kernel_fits(mesh, tokens, query_down, query_up, latent_down, rope_down, key_up, value_up, output_weight):
    S, T = mesh.shape["sp"], mesh.shape["tp"]
    H, N, V, R = query_up.shape[1], key_up.shape[2], value_up.shape[2], rope_down.shape[1]
    columns = query_down.shape[1] + latent_down.shape[1] + LANES
    return (
        S % 2 == 0 and S >= 4
        and tokens.shape[0] % 8 == 0
        and query_down.shape[0] % LANES == 0
        and query_down.shape[1] % LANES == 0
        and latent_down.shape[1] % LANES == 0
        and columns % (16 * T) == 0
        and query_up.shape[0] % 16 == 0
        and key_up.shape[0] % 16 == 0
        and output_weight.shape[1] % LANES == 0
        and H * R == LANES
        and T % 2 == 0
        and (tokens.shape[0] * T) % 32 == 0
        and R % 32 == 0
        and query_down.shape[0] == LANES
        and H * N % LANES == 0
        and N == V
    )


def rope_tables(positions, width, copies):
    h2 = width // 2
    frequency = ROPE_BASE ** (-np.arange(0, width, 2, dtype=np.float64) / width)
    angles = np.arange(positions, dtype=np.float64)[:, None] * frequency[None, :]
    cosine = np.tile(np.cos(angles), (1, 2 * copies))
    sine = np.tile(np.sin(angles), (1, copies))
    return np.stack([cosine, np.concatenate([-sine, sine], axis=1)]).astype(np.float32)


def on_device(mesh, tokens, doc_ids, query_down, query_gain, query_up, latent_down, latent_gain,
              rope_down, key_up, value_up, output_weight, output_gain):
    if not kernel_fits(mesh, tokens, query_down, query_up, latent_down, rope_down, key_up, value_up, output_weight):
        return plain_layer(tokens, doc_ids, query_down, query_gain, query_up, latent_down, latent_gain,
                           rope_down, key_up, value_up, output_weight, output_gain)
    S, T = mesh.shape["sp"], mesh.shape["tp"]
    H, N, V, R = query_up.shape[1], key_up.shape[2], value_up.shape[2], rope_down.shape[1]
    QW, LW = query_down.shape[1], latent_down.shape[1]
    rows, width = tokens.shape
    span = rows * T
    share = (QW + LANES + LW) // T
    table = jnp.asarray(rope_tables(S * span, R, H))
    sizes = dict(S=S, T=T, H=H, N=N, V=V, R=R, QW=QW, LW=LW)
    vmem = pl.BlockSpec(memory_space=pltpu.VMEM)
    bf16 = jnp.bfloat16
    sem = pltpu.SemaphoreType.DMA
    hbm = pl.BlockSpec(memory_space=pltpu.HBM)
    wq = (query_up.shape[0], H * (N + R))
    wkv = (2 * key_up.shape[0], H * N)
    return pl.pallas_call(
        functools.partial(layer_kernel, sizes),
        out_shape=jax.ShapeDtypeStruct((rows, width), bf16),
        in_specs=[hbm] * 13,
        out_specs=vmem,
        scratch_shapes=[
            pltpu.VMEM((1, span), jnp.int32),
            pltpu.VMEM((1, QW), jnp.float32),
            pltpu.VMEM((1, LW), jnp.float32),
            pltpu.VMEM((1, width), jnp.float32),
            pltpu.VMEM(tokens.shape, bf16),
            pltpu.VMEM(query_down.shape, bf16),
            pltpu.VMEM(latent_down.shape, bf16),
            pltpu.VMEM(rope_down.shape[::-1], bf16),
            pltpu.VMEM(query_up.shape, bf16),
            pltpu.VMEM(key_up.shape, bf16),
            pltpu.VMEM(value_up.shape, bf16),
            pltpu.VMEM(output_weight.shape, bf16),
            pltpu.VMEM((2, span, LANES), jnp.float32),
            pltpu.VMEM((QW + LANES + LW, query_down.shape[0]), bf16),
            pltpu.VMEM(wq, bf16),
            pltpu.VMEM(wkv, bf16),
            pltpu.VMEM((T, rows, width), bf16),
            pltpu.VMEM((span, width), bf16),
            pltpu.VMEM((S, share, query_down.shape[0]), bf16),
            pltpu.VMEM((S,) + wq, bf16),
            pltpu.VMEM((S,) + wkv, bf16),
            pltpu.VMEM((S,) + output_weight.shape, bf16),
            pltpu.VMEM((T, span, share), bf16),
            pltpu.VMEM((span, LW + LANES), bf16),
            pltpu.VMEM((S, span, LW + LANES), bf16),
            pltpu.VMEM((T, rows, width), bf16),
            pltpu.VMEM((T - 1, rows, width), bf16),
            sem((4, S - 1)),
            sem((4, S - 1)),
            sem((S - 1,)),
            sem((S - 1,)),
            sem((S - 1,)),
            sem((S - 1,)),
            sem((T - 1,)),
            sem((T - 1,)),
            sem((T - 1,)),
            sem((T - 1,)),
            sem((T - 1,)),
            sem((T - 1,)),
            sem((13,)),
        ],
        compiler_params=pltpu.CompilerParams(
            collective_id=0, has_side_effects=True, vmem_limit_bytes=48 * 1024 * 1024),
    )(tokens, doc_ids[None, :], query_down, latent_down, rope_down.T, query_up, key_up, value_up, output_weight,
      query_gain[None, :], latent_gain[None, :], output_gain[None, :], table)


def solution(mesh):
    in_specs = (
        P(("sp", "tp"), None),
        P("sp"),
        P("sp", None),
        P(),
        P("sp", "tp", None),
        P("sp", None),
        P(),
        P("sp", None),
        P("sp", "tp", None),
        P("sp", "tp", None),
        P("tp", "sp"),
        P(),
    )
    out_specs = P(("sp", "tp"), None)
    return jax.shard_map(
        functools.partial(on_device, mesh), mesh=mesh, in_specs=in_specs, out_specs=out_specs, check_vma=False
    )
```

```python
import functools

import jax
import jax.numpy as jnp
import numpy as np
from jax import lax
from jax.experimental import pallas as pl
from jax.experimental.pallas import tpu as pltpu
from jax.sharding import PartitionSpec as P

ROPE_BASE = 10000.0
EPS = 1e-06
MASKED = -1e30


def folded(value, axis, dim, update, carry):
    whole = jax.tree.map(lambda part: lax.all_gather(part, axis, axis=dim, tiled=True), value)
    return update(carry, whole, jnp.int32(0))


def gathered_then(share, axis, dim, apply):
    everything = lax.all_gather(share, axis, axis=dim, tiled=True)
    return apply(everything, jnp.int32(0))


def for_sending(value):
    def short(part):
        return part.astype(jnp.bfloat16) if part.dtype == jnp.float32 else part

    return jax.tree.map(short, value)


def own_rows(term, extent, axis):
    whole = term(jnp.int32(0), extent * lax.axis_size(axis)).astype(jnp.bfloat16)
    return lax.psum_scatter(whole, axis, scatter_dimension=0, tiled=True).astype(jnp.float32)


def normalize(values, gain_vec):
    return values * lax.rsqrt(jnp.mean(values * values, axis=-1, keepdims=True) + EPS) * gain_vec


def rotate(rope_part, position):
    half_width = rope_part.shape[-1] // 2
    frequency = ROPE_BASE ** (
        -jnp.arange(0, 2 * half_width, 2, dtype=jnp.float32) / (2 * half_width)
    )
    angles = position.astype(jnp.float32)[:, None] * frequency[None, :]
    cosine = jnp.cos(angles)
    sine_part = jnp.sin(angles)
    if rope_part.ndim == 3:
        cosine = cosine[:, None, :]
        sine_part = sine_part[:, None, :]
    first_half = rope_part[..., :half_width]
    second_half = rope_part[..., half_width:]
    return jnp.concatenate(
        [
            first_half * cosine - second_half * sine_part,
            first_half * sine_part + second_half * cosine,
        ],
        axis=-1,
    )


def plain_layer(
    tokens,
    doc_ids,
    query_down,
    query_gain,
    query_up,
    latent_down,
    latent_gain,
    rope_down,
    key_up,
    value_up,
    output_weight,
    output_gain,
):
    row_count = tokens.shape[0]
    key_span = doc_ids.shape[0]
    query_width = query_down.shape[1]
    latent_width = latent_down.shape[1]
    rope_width = rope_down.shape[1]
    local_heads = query_up.shape[1]
    head_width = query_up.shape[2]
    nope_width = key_up.shape[2]
    value_width = value_up.shape[2]

    def down_term(total_now, weight_rows, first_row):
        columns = lax.dynamic_slice_in_dim(tokens, first_row, weight_rows.shape[0], 1)
        return total_now + jnp.dot(columns, weight_rows, preferred_element_type=jnp.float32)

    empty_query = jnp.zeros((row_count, query_width), jnp.float32)
    empty_latent = jnp.zeros((row_count, latent_width), jnp.float32)
    empty_rope = jnp.zeros((row_count, rope_width), jnp.float32)
    query_sum = folded(query_down, "sp", 0, down_term, empty_query)
    latent_sum = folded(latent_down, "sp", 0, down_term, empty_latent)
    rope_sum = folded(rope_down, "sp", 0, down_term, empty_rope)
    query_lat = normalize(query_sum, query_gain).astype(jnp.bfloat16)
    kv_lat = normalize(latent_sum, latent_gain).astype(jnp.bfloat16)
    own_position = lax.axis_index(("sp", "tp")) * row_count + lax.iota(jnp.int32, row_count)
    rope_keys = rotate(rope_sum, own_position).astype(jnp.bfloat16)
    query_full, key_full, value_full = (
        lax.all_gather(query_up, "sp", axis=0, tiled=True),
        lax.all_gather(key_up, "sp", axis=0, tiled=True),
        lax.all_gather(value_up, "sp", axis=0, tiled=True),
    )
    flat_width = local_heads * head_width
    query_matrix = query_full.reshape(query_width, flat_width)
    block_offset = lax.axis_index("sp") * key_span

    def project(latent_rows, first_row):
        piece_rows = latent_rows.shape[0]
        raw_query = jnp.dot(
            latent_rows[:, :query_width], query_matrix, preferred_element_type=jnp.float32
        ).reshape(piece_rows, local_heads, head_width)
        position = block_offset + first_row + lax.iota(jnp.int32, piece_rows)
        turned = jnp.concatenate(
            [raw_query[..., :nope_width], rotate(raw_query[..., nope_width:], position)], axis=-1
        )
        return jnp.concatenate(
            [
                turned.astype(jnp.bfloat16).reshape(piece_rows, flat_width),
                latent_rows[:, query_width:],
            ],
            axis=1,
        )

    packed = jnp.concatenate([query_lat, kv_lat, rope_keys], axis=1)
    gathered = gathered_then(packed, "tp", 0, project)
    queries = gathered[:, :flat_width].reshape(key_span, local_heads, head_width)
    my_ids = doc_ids.astype(jnp.bfloat16)
    key_rows = jnp.concatenate([gathered[:, flat_width:], my_ids[:, None]], axis=1)
    query_nope = queries[..., :nope_width]
    query_rope = queries[..., nope_width:]
    score_scale = head_width ** (-0.5)
    absorbed = jnp.einsum("qhe,rhe->qhr", query_nope, key_full, preferred_element_type=jnp.float32)

    def block_scores(latent_part, rope_part):
        latent_float = latent_part.astype(jnp.float32)
        scores = jnp.einsum("qhr,kr->qhk", absorbed, latent_float, precision=lax.Precision.HIGHEST)
        scores = scores + jnp.einsum(
            "qhe,ke->qhk", query_rope, rope_part, preferred_element_type=jnp.float32
        )
        return (scores * score_scale, latent_float)

    def finish(averaged):
        return jnp.einsum(
            "qhr,rhv->qhv",
            averaged,
            value_full.astype(jnp.float32),
            precision=lax.Precision.HIGHEST,
        )

    def scan_step(state_now, block_keys):
        row_peak, row_total, running = state_now
        latent_part = block_keys[:, :latent_width]
        rope_part = block_keys[:, latent_width : latent_width + rope_width]
        block_ids = block_keys[:, latent_width + rope_width]
        scores, value_part = block_scores(latent_part, rope_part)
        same_doc = my_ids[:, None, None] == block_ids[None, None, :]
        peak_new = jnp.maximum(row_peak, jnp.max(jnp.where(same_doc, scores, MASKED), axis=-1))
        soft_weights = jnp.where(same_doc, jnp.exp(scores - peak_new[..., None]), 0.0)
        factor = jnp.exp(row_peak - peak_new)
        if value_part.ndim == 3:
            contrib = jnp.einsum(
                "qhk,khv->qhv", soft_weights, value_part, precision=lax.Precision.HIGHEST
            )
        else:
            contrib = jnp.einsum(
                "qhk,kv->qhv", soft_weights, value_part, precision=lax.Precision.HIGHEST
            )
        next_state = (
            peak_new,
            row_total * factor + jnp.sum(soft_weights, axis=-1),
            running * factor[..., None] + contrib,
        )
        return (next_state, None)

    def fold_keys(state_now, key_piece, first_row):
        key_blocks = key_piece.reshape(key_piece.shape[0] // key_span, key_span, key_piece.shape[1])
        return lax.scan(scan_step, state_now, key_blocks)[0]

    start_state = (
        jnp.full((key_span, local_heads), MASKED, jnp.float32),
        jnp.zeros((key_span, local_heads), jnp.float32),
        jnp.zeros((key_span, local_heads, latent_width), jnp.float32),
    )
    row_peak, row_total, running = folded(for_sending(key_rows), "sp", 0, fold_keys, start_state)
    averaged = running / row_total[..., None]
    attended = finish(averaged).astype(jnp.bfloat16).reshape(key_span, local_heads * value_width)
    out_full = lax.all_gather(output_weight, "sp", axis=1, tiled=True)

    def out_term(first_row, row_span):
        row_block = lax.dynamic_slice_in_dim(attended, first_row, row_span, 0)
        return jnp.dot(row_block, out_full, preferred_element_type=jnp.float32)

    mixed = own_rows(out_term, row_count, "tp")
    return normalize(mixed, output_gain).astype(jnp.bfloat16)


MESH = pl.DeviceIdType.MESH
LANES = 128
PENALTY = 1e6


def nt_dot(left, right):
    return lax.dot_general(
        left, right, (((1,), (1,)), ((), ())), preferred_element_type=jnp.float32
    )


def nn_dot(left, right):
    return jnp.dot(left, right, preferred_element_type=jnp.float32)


def layer_kernel(
    sizes,
    tok_in,
    ids_in,
    query_down,
    latent_down,
    rope_down,
    query_up,
    key_up,
    value_up,
    out_in,
    query_gain_in,
    latent_gain_in,
    output_gain_in,
    table,
    out,
    ids,
    query_gain,
    latent_gain,
    output_gain,
    tok,
    query_down_buf,
    latent_down_buf,
    rope_down_buf,
    query_up_buf,
    key_up_buf,
    value_up_buf,
    out_w,
    table_buf,
    pack,
    query_pack,
    kv_pack,
    tok_all,
    tok_flat,
    down_all,
    query_all,
    kvup_all,
    out_all,
    raw_all,
    row_buf,
    row_all,
    part_buf,
    part_all,
    weight_send,
    weight_recv,
    row_send,
    row_recv,
    core_send,
    core_recv,
    tok_send,
    tok_recv,
    raw_send,
    raw_recv,
    part_send,
    part_recv,
    local_sem,
):
    S, T, H, N, V, R = (sizes[k] for k in ("S", "T", "H", "N", "V", "R"))
    QW, LW = sizes["QW"], sizes["LW"]
    f32, bf16 = jnp.float32, jnp.bfloat16
    rows = tok.shape[0]
    span = rows * T
    half = S // 2
    h2 = R // 2
    depth = query_down.shape[0]
    share = down_all.shape[1]
    s = lax.axis_index("sp")
    t = lax.axis_index("tp")
    pair = s + 1 - 2 * (s % 2)
    twin = t + 1 - 2 * (t % 2)

    def line(k):
        return (s + 2 * k) % S

    def mate(k):
        return (t + k) % T

    def remote(src, dst, send, recv, sp, tp):
        return pltpu.make_async_remote_copy(
            src_ref=src, dst_ref=dst, send_sem=send, recv_sem=recv,
            device_id={"sp": sp, "tp": tp}, device_id_type=MESH)

    barrier = pltpu.get_barrier_semaphore()
    for k in range(1, half):
        pl.semaphore_signal(barrier, inc=1, device_id={"sp": line(k), "tp": t}, device_id_type=MESH)
    pl.semaphore_signal(barrier, inc=1, device_id={"sp": pair, "tp": t}, device_id_type=MESH)
    for k in range(1, T):
        pl.semaphore_signal(barrier, inc=1, device_id={"sp": s, "tp": mate(k)}, device_id_type=MESH)

    loads = [
        (query_down, query_down_buf),
        (latent_down, latent_down_buf),
        (rope_down, rope_down_buf),
        (tok_in, tok),
        (query_up, query_up_buf),
        (key_up, key_up_buf),
        (value_up, value_up_buf),
        (out_in, out_w),
        (table.at[:, pl.ds(pl.multiple_of(s * span, 8), span)], table_buf),
        (ids_in, ids),
        (query_gain_in, query_gain),
        (latent_gain_in, latent_gain),
        (output_gain_in, output_gain),
    ]
    copies = []
    for i, (src, dst) in enumerate(loads):
        copy = pltpu.make_async_copy(src, dst, local_sem.at[i])
        copy.start()
        copies.append(copy)

    for copy in copies[:3]:
        copy.wait()
    pack[:QW] = query_down_buf[...].astype(f32).T.astype(bf16)
    pack[QW + LANES:] = latent_down_buf[...].astype(f32).T.astype(bf16)
    rope_cols = rope_down_buf[...].astype(f32)
    gap = jnp.zeros((LANES // 2 - h2, depth), f32)
    pack[QW:QW + LANES] = jnp.concatenate(
        [rope_cols[:h2], gap, rope_cols[h2:R], gap], axis=0).astype(bf16)
    down = pack.at[pl.ds(pl.multiple_of(t * share, 16), share)]
    copies[3].wait()
    pl.semaphore_wait(barrier, half - 1 + 1 + T - 1)

    def spread(own, view, send, recv):
        sent = []
        for k in range(1, half):
            sent.append(remote(own, view(s), send.at[k - 1], recv.at[k - 1], line(k), t))
        sent.append(remote(own, view(s), send.at[half - 1], recv.at[half - 1], pair, t))
        for copy in sent:
            copy.start()
        return sent

    def landed(view, send, recv, slot):
        remote(view(s), view(s), send.at[slot], recv.at[slot], pair, t).wait_recv()

    def pass_on(view, send, recv, sent, k):
        landed(view, send, recv, k - 1)
        block = line(half - k)
        slot = half - 1 + k
        copy = remote(view(block), view(block), send.at[slot], recv.at[slot], pair, t)
        copy.start()
        sent.append(copy)
        return block

    def pair_block(j):
        return (pair + 2 * (half - j)) % S

    def to_mates(src_of, dst, send, recv):
        sent = [remote(src_of(k), dst, send.at[k - 1], recv.at[k - 1], s, mate(k)) for k in range(1, T)]
        for copy in sent:
            copy.start()
        return sent

    wholes = [down_all, query_all, kvup_all, out_all]
    owns = [down, query_pack, kv_pack, out_w]
    views = [lambda i, w=w: w.at[i] for w in wholes]
    weight_sent = [[], [], [], []]

    def begin(i):
        weight_sent[i] += spread(owns[i], views[i], weight_send.at[i], weight_recv.at[i])

    def relay(i, then=None):
        for k in range(1, half):
            block = pass_on(views[i], weight_send.at[i], weight_recv.at[i], weight_sent[i], k)
            if then is not None:
                then(block)

    def rest(i, then=None):
        for j in range(half):
            landed(views[i], weight_send.at[i], weight_recv.at[i], half - 1 + j)
            if then is not None:
                then(pair_block(j))

    begin(0)
    tok_sent = to_mates(lambda k: tok, tok_all.at[t], tok_send, tok_recv)
    down_all[s] = down[...]
    tok_all[t] = tok[...]

    for copy in copies[4:8]:
        copy.wait()
    query_in = [query_up_buf[:, h, :].astype(f32) for h in range(H)]
    query_pack[...] = jnp.concatenate(
        [x[:, :N] for x in query_in] + [x[:, N:N + h2] for x in query_in] + [x[:, N + h2:] for x in query_in],
        axis=1).astype(bf16)
    k_rows = key_up.shape[0]
    kv_pack[:k_rows] = jnp.concatenate([key_up_buf[:, h, :].astype(f32) for h in range(H)], axis=1).astype(bf16)
    kv_pack[k_rows:] = jnp.concatenate([value_up_buf[:, h, :].astype(f32) for h in range(H)], axis=1).astype(bf16)
    query_all[s] = query_pack[...]
    kvup_all[s] = kv_pack[...]
    out_all[s] = out_w[...]

    for copy in tok_sent:
        copy.wait_recv()
    tok_flat[...] = tok_all[...].astype(f32).reshape(span, tok.shape[1]).astype(bf16)
    total_raw = [jnp.zeros((span, share), f32)]

    def down_block(block):
        columns = tok_flat[:, pl.ds(pl.multiple_of(block * depth, LANES), depth)]
        total_raw[0] = total_raw[0] + nt_dot(columns, down_all[block])

    down_block(s)
    relay(0, down_block)
    begin(1)
    begin(2)
    rest(0, down_block)
    raw_all[t] = total_raw[0].astype(bf16)
    raw_sent = to_mates(lambda k: raw_all.at[t], raw_all.at[t], raw_send, raw_recv)
    for copy in copies[8:]:
        copy.wait()
    cosine = table_buf[0]
    sine = table_buf[1]
    lane = lax.broadcasted_iota(jnp.int32, (span, LANES), 1)
    padded = -(-span // LANES) * LANES
    id_row = jnp.concatenate([ids[...].astype(f32), jnp.zeros((1, padded - span), f32)], axis=1)
    own_id = jnp.broadcast_to(id_row, (LANES, padded)).T[:span]
    id_lane = (lane - h2).astype(f32)
    is_id = (lane >= h2) & (lane < LANES // 2)

    for copy in raw_sent:
        copy.wait_recv()
    whole_raw = jnp.concatenate([raw_all[j].astype(f32) for j in range(T)], axis=1)
    query_raw = whole_raw[:, :QW]
    rope_raw = whole_raw[:, QW:QW + LANES]
    latent_raw = whole_raw[:, QW + LANES:QW + LANES + LW]

    def turn(x):
        return x * cosine + pltpu.roll(x, LANES // 2, 1) * sine

    key_marks = jnp.where(is_id & (id_lane != own_id), -1.0, 0.0)
    row_buf[:, :LW] = normalize(latent_raw, latent_gain[...]).astype(bf16)
    row_buf[:, LW:] = jnp.where(is_id, key_marks, turn(rope_raw)).astype(bf16)
    part_rows = span // 2
    mine = pl.ds(pl.multiple_of((t % 2) * part_rows, 16), part_rows)

    def row_view(i):
        return row_all.at[i, mine]

    row_sent = spread(row_buf.at[mine], row_view, row_send, row_recv)
    relay(1)
    relay(2)
    begin(3)

    query_lat = normalize(query_raw, query_gain[...]).astype(bf16)
    rest(1)
    queries = nn_dot(query_lat, query_all[...].reshape(QW, query_pack.shape[1]))
    nope = queries[:, :H * N].astype(bf16)
    rope = turn(queries[:, H * N:])
    nope_lane = lax.broadcasted_iota(jnp.int32, (span, H * N), 1)
    spread_nope = jnp.concatenate(
        [jnp.where((nope_lane >= h * N) & (nope_lane < (h + 1) * N), nope, jnp.zeros_like(nope)) for h in range(H)],
        axis=0)
    is_rope = (lane < h2) | ((lane >= LANES // 2) & (lane < LANES // 2 + h2))
    query_marks = jnp.where(is_id & (id_lane == own_id), PENALTY, 0.0)
    spread_rope = jnp.concatenate(
        [jnp.where(is_rope, rope if h == 0 else pltpu.roll(rope, LANES - h * h2, 1), query_marks).astype(bf16) for h in range(H)],
        axis=0)
    core_sent = []

    def to_twin(block, slot):
        copy = remote(row_view(block), row_view(block), core_send.at[slot], core_recv.at[slot], s, twin)
        copy.start()
        core_sent.append(copy)

    rest(2)
    key_matrix = kvup_all[:, :k_rows, :].reshape(LW, kv_pack.shape[1])
    value_matrix = kvup_all[:, k_rows:, :].reshape(LW, kv_pack.shape[1])
    absorbed = nt_dot(spread_nope, key_matrix).astype(bf16)
    wide_query = jnp.concatenate([absorbed, spread_rope], axis=1)
    scale = (N + R) ** (-0.5)

    def block_scores(key_rows):
        return nt_dot(wide_query, key_rows) * scale

    first = block_scores(row_buf[...])
    peak = jnp.max(first, axis=-1, keepdims=True)
    first = jnp.exp(first - peak)
    state = [peak, jnp.sum(first, axis=-1, keepdims=True), nn_dot(first.astype(bf16), row_buf[:, :LW])]

    def fold(blocks):
        key_rows = jnp.concatenate([row_all[b].astype(f32) for b in blocks], axis=0).astype(bf16)
        scores = block_scores(key_rows)
        peak, total, running = state
        peak_new = jnp.maximum(peak, jnp.max(scores, axis=-1, keepdims=True))
        factor = jnp.exp(peak - peak_new)
        weights = jnp.exp(scores - peak_new)
        state[0] = peak_new
        state[1] = total * factor + jnp.sum(weights, axis=-1, keepdims=True)
        state[2] = running * factor + nn_dot(weights.astype(bf16), key_rows[:, :LW])

    blocks = [pass_on(row_view, row_send, row_recv, row_sent, k) for k in range(1, half)]
    for slot, block in enumerate(blocks):
        to_twin(block, slot)
    for j in range(half):
        landed(row_view, row_send, row_recv, half - 1 + j)
        to_twin(pair_block(j), half - 1 + j)
    for copy in core_sent[:half - 1]:
        copy.wait_recv()
    fold(blocks)
    for copy in core_sent[half - 1:]:
        copy.wait_recv()
    fold([pair_block(j) for j in range(half)])
    relay(3)
    averaged = state[2] / state[1]
    everything = nn_dot(averaged.astype(bf16), value_matrix)
    value_lane = lax.broadcasted_iota(jnp.int32, (span, H * V), 1)
    attended = jnp.zeros((span, H * V), f32)
    for h in range(H):
        attended = jnp.where(
            (value_lane >= h * V) & (value_lane < (h + 1) * V), everything[h * span:(h + 1) * span], attended)
    attended = attended.astype(bf16)
    rest(3)
    columns = out_w.shape[1]
    for j in range(S):
        part = nn_dot(attended, out_all[j])
        for i in range(T):
            part_buf[i, :, j * columns:(j + 1) * columns] = part[i * rows:(i + 1) * rows].astype(bf16)
    part_sent = []
    for k in range(1, T):
        copy = remote(part_buf.at[mate(k)], part_all.at[k - 1], part_send.at[k - 1], part_recv.at[k - 1], s, mate(k))
        copy.start()
        part_sent.append(copy)
    mixed = part_buf[t].astype(f32)
    for k in range(1, T):
        part_sent[k - 1].wait_recv()
        mixed = mixed + part_all[k - 1].astype(f32)
    out[...] = normalize(mixed, output_gain[...]).astype(bf16)
    for copy in tok_sent + raw_sent + row_sent + core_sent + part_sent + [c for group in weight_sent for c in group]:
        copy.wait_send()


def kernel_fits(mesh, tokens, query_down, query_up, latent_down, rope_down, key_up, value_up, output_weight):
    S, T = mesh.shape["sp"], mesh.shape["tp"]
    H, N, V, R = query_up.shape[1], key_up.shape[2], value_up.shape[2], rope_down.shape[1]
    columns = query_down.shape[1] + latent_down.shape[1] + LANES
    return (
        S % 2 == 0 and S >= 4
        and tokens.shape[0] % 8 == 0
        and query_down.shape[0] % LANES == 0
        and query_down.shape[1] % LANES == 0
        and latent_down.shape[1] % LANES == 0
        and columns % (16 * T) == 0
        and query_up.shape[0] % 16 == 0
        and key_up.shape[0] % 16 == 0
        and output_weight.shape[1] % LANES == 0
        and H * R == LANES
        and T % 2 == 0
        and (tokens.shape[0] * T) % 32 == 0
        and R % 32 == 0
        and query_down.shape[0] == LANES
        and H * N % LANES == 0
        and N == V
    )


def rope_tables(positions, width, copies):
    h2 = width // 2
    frequency = ROPE_BASE ** (-np.arange(0, width, 2, dtype=np.float64) / width)
    angles = np.arange(positions, dtype=np.float64)[:, None] * frequency[None, :]
    cosine = np.tile(np.cos(angles), (1, 2 * copies))
    sine = np.tile(np.sin(angles), (1, copies))
    return np.stack([cosine, np.concatenate([-sine, sine], axis=1)]).astype(np.float32)


def on_device(mesh, tokens, doc_ids, query_down, query_gain, query_up, latent_down, latent_gain,
              rope_down, key_up, value_up, output_weight, output_gain):
    if not kernel_fits(mesh, tokens, query_down, query_up, latent_down, rope_down, key_up, value_up, output_weight):
        return plain_layer(tokens, doc_ids, query_down, query_gain, query_up, latent_down, latent_gain,
                           rope_down, key_up, value_up, output_weight, output_gain)
    S, T = mesh.shape["sp"], mesh.shape["tp"]
    H, N, V, R = query_up.shape[1], key_up.shape[2], value_up.shape[2], rope_down.shape[1]
    QW, LW = query_down.shape[1], latent_down.shape[1]
    rows, width = tokens.shape
    span = rows * T
    share = (QW + LANES + LW) // T
    table = jnp.asarray(rope_tables(S * span, R, H))
    sizes = dict(S=S, T=T, H=H, N=N, V=V, R=R, QW=QW, LW=LW)
    vmem = pl.BlockSpec(memory_space=pltpu.VMEM)
    bf16 = jnp.bfloat16
    sem = pltpu.SemaphoreType.DMA
    hbm = pl.BlockSpec(memory_space=pltpu.HBM)
    wq = (query_up.shape[0], H * (N + R))
    wkv = (2 * key_up.shape[0], H * N)
    return pl.pallas_call(
        functools.partial(layer_kernel, sizes),
        out_shape=jax.ShapeDtypeStruct((rows, width), bf16),
        in_specs=[hbm] * 13,
        out_specs=vmem,
        scratch_shapes=[
            pltpu.VMEM((1, span), jnp.int32),
            pltpu.VMEM((1, QW), jnp.float32),
            pltpu.VMEM((1, LW), jnp.float32),
            pltpu.VMEM((1, width), jnp.float32),
            pltpu.VMEM(tokens.shape, bf16),
            pltpu.VMEM(query_down.shape, bf16),
            pltpu.VMEM(latent_down.shape, bf16),
            pltpu.VMEM(rope_down.shape[::-1], bf16),
            pltpu.VMEM(query_up.shape, bf16),
            pltpu.VMEM(key_up.shape, bf16),
            pltpu.VMEM(value_up.shape, bf16),
            pltpu.VMEM(output_weight.shape, bf16),
            pltpu.VMEM((2, span, LANES), jnp.float32),
            pltpu.VMEM((QW + LANES + LW, query_down.shape[0]), bf16),
            pltpu.VMEM(wq, bf16),
            pltpu.VMEM(wkv, bf16),
            pltpu.VMEM((T, rows, width), bf16),
            pltpu.VMEM((span, width), bf16),
            pltpu.VMEM((S, share, query_down.shape[0]), bf16),
            pltpu.VMEM((S,) + wq, bf16),
            pltpu.VMEM((S,) + wkv, bf16),
            pltpu.VMEM((S,) + output_weight.shape, bf16),
            pltpu.VMEM((T, span, share), bf16),
            pltpu.VMEM((span, LW + LANES), bf16),
            pltpu.VMEM((S, span, LW + LANES), bf16),
            pltpu.VMEM((T, rows, width), bf16),
            pltpu.VMEM((T - 1, rows, width), bf16),
            sem((4, S - 1)),
            sem((4, S - 1)),
            sem((S - 1,)),
            sem((S - 1,)),
            sem((S - 1,)),
            sem((S - 1,)),
            sem((T - 1,)),
            sem((T - 1,)),
            sem((T - 1,)),
            sem((T - 1,)),
            sem((T - 1,)),
            sem((T - 1,)),
            sem((13,)),
        ],
        compiler_params=pltpu.CompilerParams(
            collective_id=0, has_side_effects=True, vmem_limit_bytes=67043328),
    )(tokens, doc_ids[None, :], query_down, latent_down, rope_down.T, query_up, key_up, value_up, output_weight,
      query_gain[None, :], latent_gain[None, :], output_gain[None, :], table)


def solution(mesh):
    in_specs = (
        P(("sp", "tp"), None),
        P("sp"),
        P("sp", None),
        P(),
        P("sp", "tp", None),
        P("sp", None),
        P(),
        P("sp", None),
        P("sp", "tp", None),
        P("sp", "tp", None),
        P("tp", "sp"),
        P(),
    )
    out_specs = P(("sp", "tp"), None)
    return jax.shard_map(
        functools.partial(on_device, mesh), mesh=mesh, in_specs=in_specs, out_specs=out_specs, check_vma=False
    )
```

```python
import functools

import jax
import jax.numpy as jnp
import numpy as np
from jax import lax
from jax.experimental import pallas as pl
from jax.experimental.pallas import tpu as pltpu
from jax.sharding import PartitionSpec as P

ROPE_BASE = 10000.0
EPS = 1e-06
MASKED = -1e30


def folded(value, axis, dim, update, carry):
    whole = jax.tree.map(lambda part: lax.all_gather(part, axis, axis=dim, tiled=True), value)
    return update(carry, whole, jnp.int32(0))


def gathered_then(share, axis, dim, apply):
    everything = lax.all_gather(share, axis, axis=dim, tiled=True)
    return apply(everything, jnp.int32(0))


def for_sending(value):
    def short(part):
        return part.astype(jnp.bfloat16) if part.dtype == jnp.float32 else part

    return jax.tree.map(short, value)


def own_rows(term, extent, axis):
    whole = term(jnp.int32(0), extent * lax.axis_size(axis)).astype(jnp.bfloat16)
    return lax.psum_scatter(whole, axis, scatter_dimension=0, tiled=True).astype(jnp.float32)


def normalize(values, gain_vec):
    return values * lax.rsqrt(jnp.mean(values * values, axis=-1, keepdims=True) + EPS) * gain_vec


def rotate(rope_part, position):
    half_width = rope_part.shape[-1] // 2
    frequency = ROPE_BASE ** (
        -jnp.arange(0, 2 * half_width, 2, dtype=jnp.float32) / (2 * half_width)
    )
    angles = position.astype(jnp.float32)[:, None] * frequency[None, :]
    cosine = jnp.cos(angles)
    sine_part = jnp.sin(angles)
    if rope_part.ndim == 3:
        cosine = cosine[:, None, :]
        sine_part = sine_part[:, None, :]
    first_half = rope_part[..., :half_width]
    second_half = rope_part[..., half_width:]
    return jnp.concatenate(
        [
            first_half * cosine - second_half * sine_part,
            first_half * sine_part + second_half * cosine,
        ],
        axis=-1,
    )


def plain_layer(
    tokens,
    doc_ids,
    query_down,
    query_gain,
    query_up,
    latent_down,
    latent_gain,
    rope_down,
    key_up,
    value_up,
    output_weight,
    output_gain,
):
    row_count = tokens.shape[0]
    key_span = doc_ids.shape[0]
    query_width = query_down.shape[1]
    latent_width = latent_down.shape[1]
    rope_width = rope_down.shape[1]
    local_heads = query_up.shape[1]
    head_width = query_up.shape[2]
    nope_width = key_up.shape[2]
    value_width = value_up.shape[2]

    def down_term(total_now, weight_rows, first_row):
        columns = lax.dynamic_slice_in_dim(tokens, first_row, weight_rows.shape[0], 1)
        return total_now + jnp.dot(columns, weight_rows, preferred_element_type=jnp.float32)

    empty_query = jnp.zeros((row_count, query_width), jnp.float32)
    empty_latent = jnp.zeros((row_count, latent_width), jnp.float32)
    empty_rope = jnp.zeros((row_count, rope_width), jnp.float32)
    query_sum = folded(query_down, "sp", 0, down_term, empty_query)
    latent_sum = folded(latent_down, "sp", 0, down_term, empty_latent)
    rope_sum = folded(rope_down, "sp", 0, down_term, empty_rope)
    query_lat = normalize(query_sum, query_gain).astype(jnp.bfloat16)
    kv_lat = normalize(latent_sum, latent_gain).astype(jnp.bfloat16)
    own_position = lax.axis_index(("sp", "tp")) * row_count + lax.iota(jnp.int32, row_count)
    rope_keys = rotate(rope_sum, own_position).astype(jnp.bfloat16)
    query_full, key_full, value_full = (
        lax.all_gather(query_up, "sp", axis=0, tiled=True),
        lax.all_gather(key_up, "sp", axis=0, tiled=True),
        lax.all_gather(value_up, "sp", axis=0, tiled=True),
    )
    flat_width = local_heads * head_width
    query_matrix = query_full.reshape(query_width, flat_width)
    block_offset = lax.axis_index("sp") * key_span

    def project(latent_rows, first_row):
        piece_rows = latent_rows.shape[0]
        raw_query = jnp.dot(
            latent_rows[:, :query_width], query_matrix, preferred_element_type=jnp.float32
        ).reshape(piece_rows, local_heads, head_width)
        position = block_offset + first_row + lax.iota(jnp.int32, piece_rows)
        turned = jnp.concatenate(
            [raw_query[..., :nope_width], rotate(raw_query[..., nope_width:], position)], axis=-1
        )
        return jnp.concatenate(
            [
                turned.astype(jnp.bfloat16).reshape(piece_rows, flat_width),
                latent_rows[:, query_width:],
            ],
            axis=1,
        )

    packed = jnp.concatenate([query_lat, kv_lat, rope_keys], axis=1)
    gathered = gathered_then(packed, "tp", 0, project)
    queries = gathered[:, :flat_width].reshape(key_span, local_heads, head_width)
    my_ids = doc_ids.astype(jnp.bfloat16)
    key_rows = jnp.concatenate([gathered[:, flat_width:], my_ids[:, None]], axis=1)
    query_nope = queries[..., :nope_width]
    query_rope = queries[..., nope_width:]
    score_scale = head_width ** (-0.5)
    absorbed = jnp.einsum("qhe,rhe->qhr", query_nope, key_full, preferred_element_type=jnp.float32)

    def block_scores(latent_part, rope_part):
        latent_float = latent_part.astype(jnp.float32)
        scores = jnp.einsum("qhr,kr->qhk", absorbed, latent_float, precision=lax.Precision.HIGHEST)
        scores = scores + jnp.einsum(
            "qhe,ke->qhk", query_rope, rope_part, preferred_element_type=jnp.float32
        )
        return (scores * score_scale, latent_float)

    def finish(averaged):
        return jnp.einsum(
            "qhr,rhv->qhv",
            averaged,
            value_full.astype(jnp.float32),
            precision=lax.Precision.HIGHEST,
        )

    def scan_step(state_now, block_keys):
        row_peak, row_total, running = state_now
        latent_part = block_keys[:, :latent_width]
        rope_part = block_keys[:, latent_width : latent_width + rope_width]
        block_ids = block_keys[:, latent_width + rope_width]
        scores, value_part = block_scores(latent_part, rope_part)
        same_doc = my_ids[:, None, None] == block_ids[None, None, :]
        peak_new = jnp.maximum(row_peak, jnp.max(jnp.where(same_doc, scores, MASKED), axis=-1))
        soft_weights = jnp.where(same_doc, jnp.exp(scores - peak_new[..., None]), 0.0)
        factor = jnp.exp(row_peak - peak_new)
        if value_part.ndim == 3:
            contrib = jnp.einsum(
                "qhk,khv->qhv", soft_weights, value_part, precision=lax.Precision.HIGHEST
            )
        else:
            contrib = jnp.einsum(
                "qhk,kv->qhv", soft_weights, value_part, precision=lax.Precision.HIGHEST
            )
        next_state = (
            peak_new,
            row_total * factor + jnp.sum(soft_weights, axis=-1),
            running * factor[..., None] + contrib,
        )
        return (next_state, None)

    def fold_keys(state_now, key_piece, first_row):
        key_blocks = key_piece.reshape(key_piece.shape[0] // key_span, key_span, key_piece.shape[1])
        return lax.scan(scan_step, state_now, key_blocks)[0]

    start_state = (
        jnp.full((key_span, local_heads), MASKED, jnp.float32),
        jnp.zeros((key_span, local_heads), jnp.float32),
        jnp.zeros((key_span, local_heads, latent_width), jnp.float32),
    )
    row_peak, row_total, running = folded(for_sending(key_rows), "sp", 0, fold_keys, start_state)
    averaged = running / row_total[..., None]
    attended = finish(averaged).astype(jnp.bfloat16).reshape(key_span, local_heads * value_width)
    out_full = lax.all_gather(output_weight, "sp", axis=1, tiled=True)

    def out_term(first_row, row_span):
        row_block = lax.dynamic_slice_in_dim(attended, first_row, row_span, 0)
        return jnp.dot(row_block, out_full, preferred_element_type=jnp.float32)

    mixed = own_rows(out_term, row_count, "tp")
    return normalize(mixed, output_gain).astype(jnp.bfloat16)


MESH = pl.DeviceIdType.MESH
LANES = 128
PENALTY = 1e6


def nt_dot(left, right):
    return lax.dot_general(
        left, right, (((1,), (1,)), ((), ())), preferred_element_type=jnp.float32
    )


def nn_dot(left, right):
    return jnp.dot(left, right, preferred_element_type=jnp.float32)


def layer_kernel(
    sizes,
    tok_in,
    ids_in,
    query_down,
    latent_down,
    rope_down,
    query_up,
    key_up,
    value_up,
    out_in,
    query_gain_in,
    latent_gain_in,
    output_gain_in,
    table,
    out,
    ids,
    query_gain,
    latent_gain,
    output_gain,
    tok,
    query_down_buf,
    latent_down_buf,
    rope_down_buf,
    query_up_buf,
    key_up_buf,
    value_up_buf,
    out_w,
    table_buf,
    pack,
    query_pack,
    kv_pack,
    tok_all,
    tok_flat,
    down_all,
    query_all,
    kvup_all,
    out_all,
    raw_all,
    row_buf,
    row_all,
    part_buf,
    part_all,
    weight_send,
    weight_recv,
    row_send,
    row_recv,
    core_send,
    core_recv,
    tok_send,
    tok_recv,
    raw_send,
    raw_recv,
    part_send,
    part_recv,
    local_sem,
):
    S, T, H, N, V, R = (sizes[k] for k in ("S", "T", "H", "N", "V", "R"))
    QW, LW = sizes["QW"], sizes["LW"]
    f32, bf16 = jnp.float32, jnp.bfloat16
    rows = tok.shape[0]
    span = rows * T
    half = S // 2
    h2 = R // 2
    depth = query_down.shape[0]
    share = down_all.shape[1]
    s = lax.axis_index("sp")
    t = lax.axis_index("tp")
    pair = s + 1 - 2 * (s % 2)
    twin = t + 1 - 2 * (t % 2)

    def line(k):
        return (s + 2 * k) % S

    def mate(k):
        return (t + k) % T

    def remote(src, dst, send, recv, sp, tp):
        return pltpu.make_async_remote_copy(
            src_ref=src, dst_ref=dst, send_sem=send, recv_sem=recv,
            device_id={"sp": sp, "tp": tp}, device_id_type=MESH)

    barrier = pltpu.get_barrier_semaphore()
    for k in range(1, half):
        pl.semaphore_signal(barrier, inc=1, device_id={"sp": line(k), "tp": t}, device_id_type=MESH)
    pl.semaphore_signal(barrier, inc=1, device_id={"sp": pair, "tp": t}, device_id_type=MESH)
    for k in range(1, T):
        pl.semaphore_signal(barrier, inc=1, device_id={"sp": s, "tp": mate(k)}, device_id_type=MESH)

    loads = [
        (query_down, query_down_buf),
        (latent_down, latent_down_buf),
        (rope_down, rope_down_buf),
        (tok_in, tok),
        (query_up, query_up_buf),
        (key_up, key_up_buf),
        (value_up, value_up_buf),
        (out_in, out_w),
        (table.at[:, pl.ds(pl.multiple_of(s * span, 8), span)], table_buf),
        (ids_in, ids),
        (query_gain_in, query_gain),
        (latent_gain_in, latent_gain),
        (output_gain_in, output_gain),
    ]
    copies = []
    for i, (src, dst) in enumerate(loads):
        copy = pltpu.make_async_copy(src, dst, local_sem.at[i])
        copy.start()
        copies.append(copy)

    for copy in copies[:3]:
        copy.wait()
    pack[:QW] = query_down_buf[...].astype(f32).T.astype(bf16)
    pack[QW + LANES:] = latent_down_buf[...].astype(f32).T.astype(bf16)
    rope_cols = rope_down_buf[...].astype(f32)
    gap = jnp.zeros((LANES // 2 - h2, depth), f32)
    pack[QW:QW + LANES] = jnp.concatenate(
        [rope_cols[:h2], gap, rope_cols[h2:R], gap], axis=0).astype(bf16)
    down = pack.at[pl.ds(pl.multiple_of(t * share, 16), share)]
    copies[3].wait()
    pl.semaphore_wait(barrier, half - 1 + 1 + T - 1)

    def spread(own, view, send, recv):
        sent = []
        for k in range(1, half):
            sent.append(remote(own, view(s), send.at[k - 1], recv.at[k - 1], line(k), t))
        sent.append(remote(own, view(s), send.at[half - 1], recv.at[half - 1], pair, t))
        for copy in sent:
            copy.start()
        return sent

    def landed(view, send, recv, slot):
        remote(view(s), view(s), send.at[slot], recv.at[slot], pair, t).wait_recv()

    def pass_on(view, send, recv, sent, k):
        landed(view, send, recv, k - 1)
        block = line(half - k)
        slot = half - 1 + k
        copy = remote(view(block), view(block), send.at[slot], recv.at[slot], pair, t)
        copy.start()
        sent.append(copy)
        return block

    def pair_block(j):
        return (pair + 2 * (half - j)) % S

    def to_mates(src_of, dst, send, recv):
        sent = [remote(src_of(k), dst, send.at[k - 1], recv.at[k - 1], s, mate(k)) for k in range(1, T)]
        for copy in sent:
            copy.start()
        return sent

    wholes = [down_all, query_all, kvup_all, out_all]
    owns = [down, query_pack, kv_pack, out_w]
    views = [lambda i, w=w: w.at[i] for w in wholes]
    weight_sent = [[], [], [], []]

    def begin(i):
        weight_sent[i] += spread(owns[i], views[i], weight_send.at[i], weight_recv.at[i])

    def relay(i, then=None):
        for k in range(1, half):
            block = pass_on(views[i], weight_send.at[i], weight_recv.at[i], weight_sent[i], k)
            if then is not None:
                then(block)

    def rest(i, then=None):
        for j in range(half):
            landed(views[i], weight_send.at[i], weight_recv.at[i], half - 1 + j)
            if then is not None:
                then(pair_block(j))

    begin(0)
    tok_sent = to_mates(lambda k: tok, tok_all.at[t], tok_send, tok_recv)
    down_all[s] = down[...]
    tok_all[t] = tok[...]

    for copy in copies[4:8]:
        copy.wait()
    query_in = [query_up_buf[:, h, :].astype(f32) for h in range(H)]
    query_pack[...] = jnp.concatenate(
        [x[:, :N] for x in query_in] + [x[:, N:N + h2] for x in query_in] + [x[:, N + h2:] for x in query_in],
        axis=1).astype(bf16)
    k_rows = key_up.shape[0]
    kv_pack[:k_rows] = jnp.concatenate([key_up_buf[:, h, :].astype(f32) for h in range(H)], axis=1).astype(bf16)
    kv_pack[k_rows:] = jnp.concatenate([value_up_buf[:, h, :].astype(f32) for h in range(H)], axis=1).astype(bf16)
    query_all[s] = query_pack[...]
    kvup_all[s] = kv_pack[...]
    out_all[s] = out_w[...]

    for copy in tok_sent:
        copy.wait_recv()
    tok_flat[...] = tok_all[...].astype(f32).reshape(span, tok.shape[1]).astype(bf16)
    total_raw = [jnp.zeros((span, share), f32)]

    def down_block(block):
        columns = tok_flat[:, pl.ds(pl.multiple_of(block * depth, LANES), depth)]
        total_raw[0] = total_raw[0] + nt_dot(columns, down_all[block])

    down_block(s)
    relay(0, down_block)
    begin(1)
    begin(2)
    rest(0, down_block)
    raw_all[t] = total_raw[0].astype(bf16)
    raw_sent = to_mates(lambda k: raw_all.at[t], raw_all.at[t], raw_send, raw_recv)
    for copy in copies[8:]:
        copy.wait()
    cosine = table_buf[0]
    sine = table_buf[1]
    lane = lax.broadcasted_iota(jnp.int32, (span, LANES), 1)
    padded = -(-span // LANES) * LANES
    id_row = jnp.concatenate([ids[...].astype(f32), jnp.zeros((1, padded - span), f32)], axis=1)
    own_id = jnp.broadcast_to(id_row, (LANES, padded)).T[:span]
    id_lane = (lane - h2).astype(f32)
    is_id = (lane >= h2) & (lane < LANES // 2)

    for copy in raw_sent:
        copy.wait_recv()
    whole_raw = jnp.concatenate([raw_all[j].astype(f32) for j in range(T)], axis=1)
    query_raw = whole_raw[:, :QW]
    rope_raw = whole_raw[:, QW:QW + LANES]
    latent_raw = whole_raw[:, QW + LANES:QW + LANES + LW]

    def turn(x):
        return x * cosine + pltpu.roll(x, LANES // 2, 1) * sine

    key_marks = jnp.where(is_id & (id_lane != own_id), -1.0, 0.0)
    row_buf[:, :LW] = normalize(latent_raw, latent_gain[...][None, :]).astype(bf16)
    row_buf[:, LW:] = jnp.where(is_id, key_marks, turn(rope_raw)).astype(bf16)
    part_rows = span // 2
    mine = pl.ds(pl.multiple_of((t % 2) * part_rows, 16), part_rows)

    def row_view(i):
        return row_all.at[i, mine]

    row_sent = spread(row_buf.at[mine], row_view, row_send, row_recv)
    relay(1)
    relay(2)
    begin(3)

    query_lat = normalize(query_raw, query_gain[...][None, :]).astype(bf16)
    rest(1)
    queries = nn_dot(query_lat, query_all[...].reshape(QW, query_pack.shape[1]))
    nope = queries[:, :H * N].astype(bf16)
    rope = turn(queries[:, H * N:])
    nope_lane = lax.broadcasted_iota(jnp.int32, (span, H * N), 1)
    spread_nope = jnp.concatenate(
        [jnp.where((nope_lane >= h * N) & (nope_lane < (h + 1) * N), nope, jnp.zeros_like(nope)) for h in range(H)],
        axis=0)
    is_rope = (lane < h2) | ((lane >= LANES // 2) & (lane < LANES // 2 + h2))
    query_marks = jnp.where(is_id & (id_lane == own_id), PENALTY, 0.0)
    spread_rope = jnp.concatenate(
        [jnp.where(is_rope, rope if h == 0 else pltpu.roll(rope, LANES - h * h2, 1), query_marks).astype(bf16) for h in range(H)],
        axis=0)
    core_sent = []

    def to_twin(block, slot):
        copy = remote(row_view(block), row_view(block), core_send.at[slot], core_recv.at[slot], s, twin)
        copy.start()
        core_sent.append(copy)

    rest(2)
    key_matrix = kvup_all[:, :k_rows, :].reshape(LW, kv_pack.shape[1])
    value_matrix = kvup_all[:, k_rows:, :].reshape(LW, kv_pack.shape[1])
    absorbed = nt_dot(spread_nope, key_matrix).astype(bf16)
    wide_query = jnp.concatenate([absorbed, spread_rope], axis=1)
    scale = (N + R) ** (-0.5)

    def block_scores(key_rows):
        return nt_dot(wide_query, key_rows) * scale

    first = block_scores(row_buf[...])
    peak = jnp.max(first, axis=-1, keepdims=True)
    first = jnp.exp(first - peak)
    state = [peak, jnp.sum(first, axis=-1, keepdims=True), nn_dot(first.astype(bf16), row_buf[:, :LW])]

    def fold(blocks):
        key_rows = jnp.concatenate([row_all[b] for b in blocks], axis=0)
        scores = block_scores(key_rows)
        peak, total, running = state
        peak_new = jnp.maximum(peak, jnp.max(scores, axis=-1, keepdims=True))
        factor = jnp.exp(peak - peak_new)
        weights = jnp.exp(scores - peak_new)
        state[0] = peak_new
        state[1] = total * factor + jnp.sum(weights, axis=-1, keepdims=True)
        state[2] = running * factor + nn_dot(weights.astype(bf16), key_rows[:, :LW])

    blocks = [pass_on(row_view, row_send, row_recv, row_sent, k) for k in range(1, half)]
    for slot, block in enumerate(blocks):
        to_twin(block, slot)
    landed(row_view, row_send, row_recv, half - 1)
    to_twin(pair, half - 1)
    blocks.append(pair)
    for copy in core_sent:
        copy.wait_recv()
    fold(blocks)
    for j in range(1, half):
        landed(row_view, row_send, row_recv, half - 1 + j)
        to_twin(pair_block(j), half - 1 + j)
    for copy in core_sent[half:]:
        copy.wait_recv()
    fold([pair_block(j) for j in range(1, half)])
    relay(3)
    averaged = state[2] / state[1]
    everything = nn_dot(averaged.astype(bf16), value_matrix)
    value_lane = lax.broadcasted_iota(jnp.int32, (span, H * V), 1)
    attended = jnp.zeros((span, H * V), f32)
    for h in range(H):
        attended = jnp.where(
            (value_lane >= h * V) & (value_lane < (h + 1) * V), everything[h * span:(h + 1) * span], attended)
    attended = attended.astype(bf16)
    rest(3)
    columns = out_w.shape[1]
    for j in range(S):
        part = nn_dot(attended, out_all[j])
        for i in range(T):
            part_buf[i, :, j * columns:(j + 1) * columns] = part[i * rows:(i + 1) * rows].astype(bf16)
    part_sent = []
    for k in range(1, T):
        copy = remote(part_buf.at[mate(k)], part_all.at[k - 1], part_send.at[k - 1], part_recv.at[k - 1], s, mate(k))
        copy.start()
        part_sent.append(copy)
    mixed = part_buf[t].astype(f32)
    for k in range(1, T):
        part_sent[k - 1].wait_recv()
        mixed = mixed + part_all[k - 1].astype(f32)
    out[...] = normalize(mixed, output_gain[...][None, :]).astype(bf16)
    for copy in tok_sent + raw_sent + row_sent + core_sent + part_sent + [c for group in weight_sent for c in group]:
        copy.wait_send()


def kernel_fits(mesh, tokens, query_down, query_up, latent_down, rope_down, key_up, value_up, output_weight):
    S, T = mesh.shape["sp"], mesh.shape["tp"]
    H, N, V, R = query_up.shape[1], key_up.shape[2], value_up.shape[2], rope_down.shape[1]
    columns = query_down.shape[1] + latent_down.shape[1] + LANES
    return (
        S % 2 == 0 and S >= 4
        and tokens.shape[0] % 8 == 0
        and query_down.shape[0] % LANES == 0
        and query_down.shape[1] % LANES == 0
        and latent_down.shape[1] % LANES == 0
        and columns % (16 * T) == 0
        and query_up.shape[0] % 16 == 0
        and key_up.shape[0] % 16 == 0
        and output_weight.shape[1] % LANES == 0
        and H * R == LANES
        and T % 2 == 0
        and (tokens.shape[0] * T) % 32 == 0
        and R % 32 == 0
        and query_down.shape[0] == LANES
        and H * N % LANES == 0
        and N == V
    )


def rope_tables(positions, width, copies):
    h2 = width // 2
    frequency = ROPE_BASE ** (-np.arange(0, width, 2, dtype=np.float64) / width)
    angles = np.arange(positions, dtype=np.float64)[:, None] * frequency[None, :]
    cosine = np.tile(np.cos(angles), (1, 2 * copies))
    sine = np.tile(np.sin(angles), (1, copies))
    return np.stack([cosine, np.concatenate([-sine, sine], axis=1)]).astype(np.float32)


def on_device(mesh, tokens, doc_ids, query_down, query_gain, query_up, latent_down, latent_gain,
              rope_down, key_up, value_up, output_weight, output_gain):
    if not kernel_fits(mesh, tokens, query_down, query_up, latent_down, rope_down, key_up, value_up, output_weight):
        return plain_layer(tokens, doc_ids, query_down, query_gain, query_up, latent_down, latent_gain,
                           rope_down, key_up, value_up, output_weight, output_gain)
    S, T = mesh.shape["sp"], mesh.shape["tp"]
    H, N, V, R = query_up.shape[1], key_up.shape[2], value_up.shape[2], rope_down.shape[1]
    QW, LW = query_down.shape[1], latent_down.shape[1]
    rows, width = tokens.shape
    span = rows * T
    share = (QW + LANES + LW) // T
    table = jnp.asarray(rope_tables(S * span, R, H))
    sizes = dict(S=S, T=T, H=H, N=N, V=V, R=R, QW=QW, LW=LW)
    vmem = pl.BlockSpec(memory_space=pltpu.VMEM)
    bf16 = jnp.bfloat16
    sem = pltpu.SemaphoreType.DMA
    hbm = pl.BlockSpec(memory_space=pltpu.HBM)
    wq = (query_up.shape[0], H * (N + R))
    wkv = (2 * key_up.shape[0], H * N)
    return pl.pallas_call(
        functools.partial(layer_kernel, sizes),
        out_shape=jax.ShapeDtypeStruct((rows, width), bf16),
        in_specs=[hbm] * 13,
        out_specs=vmem,
        scratch_shapes=[
            pltpu.VMEM((1, span), jnp.int32),
            pltpu.VMEM((QW,), jnp.float32),
            pltpu.VMEM((LW,), jnp.float32),
            pltpu.VMEM((width,), jnp.float32),
            pltpu.VMEM(tokens.shape, bf16),
            pltpu.VMEM(query_down.shape, bf16),
            pltpu.VMEM(latent_down.shape, bf16),
            pltpu.VMEM(rope_down.shape[::-1], bf16),
            pltpu.VMEM(query_up.shape, bf16),
            pltpu.VMEM(key_up.shape, bf16),
            pltpu.VMEM(value_up.shape, bf16),
            pltpu.VMEM(output_weight.shape, bf16),
            pltpu.VMEM((2, span, LANES), jnp.float32),
            pltpu.VMEM((QW + LANES + LW, query_down.shape[0]), bf16),
            pltpu.VMEM(wq, bf16),
            pltpu.VMEM(wkv, bf16),
            pltpu.VMEM((T, rows, width), bf16),
            pltpu.VMEM((span, width), bf16),
            pltpu.VMEM((S, share, query_down.shape[0]), bf16),
            pltpu.VMEM((S,) + wq, bf16),
            pltpu.VMEM((S,) + wkv, bf16),
            pltpu.VMEM((S,) + output_weight.shape, bf16),
            pltpu.VMEM((T, span, share), bf16),
            pltpu.VMEM((span, LW + LANES), bf16),
            pltpu.VMEM((S, span, LW + LANES), bf16),
            pltpu.VMEM((T, rows, width), bf16),
            pltpu.VMEM((T - 1, rows, width), bf16),
            sem((4, S - 1)),
            sem((4, S - 1)),
            sem((S - 1,)),
            sem((S - 1,)),
            sem((S - 1,)),
            sem((S - 1,)),
            sem((T - 1,)),
            sem((T - 1,)),
            sem((T - 1,)),
            sem((T - 1,)),
            sem((T - 1,)),
            sem((T - 1,)),
            sem((13,)),
        ],
        compiler_params=pltpu.CompilerParams(
            collective_id=0, has_side_effects=True, vmem_limit_bytes=67043328),
    )(tokens, doc_ids[None, :], query_down, latent_down, rope_down.T, query_up, key_up, value_up, output_weight,
      query_gain, latent_gain, output_gain, table)


def solution(mesh):
    in_specs = (
        P(("sp", "tp"), None),
        P("sp"),
        P("sp", None),
        P(),
        P("sp", "tp", None),
        P("sp", None),
        P(),
        P("sp", None),
        P("sp", "tp", None),
        P("sp", "tp", None),
        P("tp", "sp"),
        P(),
    )
    out_specs = P(("sp", "tp"), None)
    return jax.shard_map(
        functools.partial(on_device, mesh), mesh=mesh, in_specs=in_specs, out_specs=out_specs, check_vma=False
    )
```

```python
import functools

import jax
import jax.numpy as jnp
import numpy as np
from jax import lax
from jax.experimental import pallas as pl
from jax.experimental.pallas import tpu as pltpu
from jax.sharding import PartitionSpec as P

ROPE_BASE = 10000.0
EPS = 1e-06
MASKED = -1e30


def folded(value, axis, dim, update, carry):
    whole = jax.tree.map(lambda part: lax.all_gather(part, axis, axis=dim, tiled=True), value)
    return update(carry, whole, jnp.int32(0))


def gathered_then(share, axis, dim, apply):
    everything = lax.all_gather(share, axis, axis=dim, tiled=True)
    return apply(everything, jnp.int32(0))


def for_sending(value):
    def short(part):
        return part.astype(jnp.bfloat16) if part.dtype == jnp.float32 else part

    return jax.tree.map(short, value)


def own_rows(term, extent, axis):
    whole = term(jnp.int32(0), extent * lax.axis_size(axis)).astype(jnp.bfloat16)
    return lax.psum_scatter(whole, axis, scatter_dimension=0, tiled=True).astype(jnp.float32)


def normalize(values, gain_vec):
    return values * lax.rsqrt(jnp.mean(values * values, axis=-1, keepdims=True) + EPS) * gain_vec


def rotate(rope_part, position):
    half_width = rope_part.shape[-1] // 2
    frequency = ROPE_BASE ** (
        -jnp.arange(0, 2 * half_width, 2, dtype=jnp.float32) / (2 * half_width)
    )
    angles = position.astype(jnp.float32)[:, None] * frequency[None, :]
    cosine = jnp.cos(angles)
    sine_part = jnp.sin(angles)
    if rope_part.ndim == 3:
        cosine = cosine[:, None, :]
        sine_part = sine_part[:, None, :]
    first_half = rope_part[..., :half_width]
    second_half = rope_part[..., half_width:]
    return jnp.concatenate(
        [
            first_half * cosine - second_half * sine_part,
            first_half * sine_part + second_half * cosine,
        ],
        axis=-1,
    )


def plain_layer(
    tokens,
    doc_ids,
    query_down,
    query_gain,
    query_up,
    latent_down,
    latent_gain,
    rope_down,
    key_up,
    value_up,
    output_weight,
    output_gain,
):
    row_count = tokens.shape[0]
    key_span = doc_ids.shape[0]
    query_width = query_down.shape[1]
    latent_width = latent_down.shape[1]
    rope_width = rope_down.shape[1]
    local_heads = query_up.shape[1]
    head_width = query_up.shape[2]
    nope_width = key_up.shape[2]
    value_width = value_up.shape[2]

    def down_term(total_now, weight_rows, first_row):
        columns = lax.dynamic_slice_in_dim(tokens, first_row, weight_rows.shape[0], 1)
        return total_now + jnp.dot(columns, weight_rows, preferred_element_type=jnp.float32)

    empty_query = jnp.zeros((row_count, query_width), jnp.float32)
    empty_latent = jnp.zeros((row_count, latent_width), jnp.float32)
    empty_rope = jnp.zeros((row_count, rope_width), jnp.float32)
    query_sum = folded(query_down, "sp", 0, down_term, empty_query)
    latent_sum = folded(latent_down, "sp", 0, down_term, empty_latent)
    rope_sum = folded(rope_down, "sp", 0, down_term, empty_rope)
    query_lat = normalize(query_sum, query_gain).astype(jnp.bfloat16)
    kv_lat = normalize(latent_sum, latent_gain).astype(jnp.bfloat16)
    own_position = lax.axis_index(("sp", "tp")) * row_count + lax.iota(jnp.int32, row_count)
    rope_keys = rotate(rope_sum, own_position).astype(jnp.bfloat16)
    query_full, key_full, value_full = (
        lax.all_gather(query_up, "sp", axis=0, tiled=True),
        lax.all_gather(key_up, "sp", axis=0, tiled=True),
        lax.all_gather(value_up, "sp", axis=0, tiled=True),
    )
    flat_width = local_heads * head_width
    query_matrix = query_full.reshape(query_width, flat_width)
    block_offset = lax.axis_index("sp") * key_span

    def project(latent_rows, first_row):
        piece_rows = latent_rows.shape[0]
        raw_query = jnp.dot(
            latent_rows[:, :query_width], query_matrix, preferred_element_type=jnp.float32
        ).reshape(piece_rows, local_heads, head_width)
        position = block_offset + first_row + lax.iota(jnp.int32, piece_rows)
        turned = jnp.concatenate(
            [raw_query[..., :nope_width], rotate(raw_query[..., nope_width:], position)], axis=-1
        )
        return jnp.concatenate(
            [
                turned.astype(jnp.bfloat16).reshape(piece_rows, flat_width),
                latent_rows[:, query_width:],
            ],
            axis=1,
        )

    packed = jnp.concatenate([query_lat, kv_lat, rope_keys], axis=1)
    gathered = gathered_then(packed, "tp", 0, project)
    queries = gathered[:, :flat_width].reshape(key_span, local_heads, head_width)
    my_ids = doc_ids.astype(jnp.bfloat16)
    key_rows = jnp.concatenate([gathered[:, flat_width:], my_ids[:, None]], axis=1)
    query_nope = queries[..., :nope_width]
    query_rope = queries[..., nope_width:]
    score_scale = head_width ** (-0.5)
    absorbed = jnp.einsum("qhe,rhe->qhr", query_nope, key_full, preferred_element_type=jnp.float32)

    def block_scores(latent_part, rope_part):
        latent_float = latent_part.astype(jnp.float32)
        scores = jnp.einsum("qhr,kr->qhk", absorbed, latent_float, precision=lax.Precision.HIGHEST)
        scores = scores + jnp.einsum(
            "qhe,ke->qhk", query_rope, rope_part, preferred_element_type=jnp.float32
        )
        return (scores * score_scale, latent_float)

    def finish(averaged):
        return jnp.einsum(
            "qhr,rhv->qhv",
            averaged,
            value_full.astype(jnp.float32),
            precision=lax.Precision.HIGHEST,
        )

    def scan_step(state_now, block_keys):
        row_peak, row_total, running = state_now
        latent_part = block_keys[:, :latent_width]
        rope_part = block_keys[:, latent_width : latent_width + rope_width]
        block_ids = block_keys[:, latent_width + rope_width]
        scores, value_part = block_scores(latent_part, rope_part)
        same_doc = my_ids[:, None, None] == block_ids[None, None, :]
        peak_new = jnp.maximum(row_peak, jnp.max(jnp.where(same_doc, scores, MASKED), axis=-1))
        soft_weights = jnp.where(same_doc, jnp.exp(scores - peak_new[..., None]), 0.0)
        factor = jnp.exp(row_peak - peak_new)
        if value_part.ndim == 3:
            contrib = jnp.einsum(
                "qhk,khv->qhv", soft_weights, value_part, precision=lax.Precision.HIGHEST
            )
        else:
            contrib = jnp.einsum(
                "qhk,kv->qhv", soft_weights, value_part, precision=lax.Precision.HIGHEST
            )
        next_state = (
            peak_new,
            row_total * factor + jnp.sum(soft_weights, axis=-1),
            running * factor[..., None] + contrib,
        )
        return (next_state, None)

    def fold_keys(state_now, key_piece, first_row):
        key_blocks = key_piece.reshape(key_piece.shape[0] // key_span, key_span, key_piece.shape[1])
        return lax.scan(scan_step, state_now, key_blocks)[0]

    start_state = (
        jnp.full((key_span, local_heads), MASKED, jnp.float32),
        jnp.zeros((key_span, local_heads), jnp.float32),
        jnp.zeros((key_span, local_heads, latent_width), jnp.float32),
    )
    row_peak, row_total, running = folded(for_sending(key_rows), "sp", 0, fold_keys, start_state)
    averaged = running / row_total[..., None]
    attended = finish(averaged).astype(jnp.bfloat16).reshape(key_span, local_heads * value_width)
    out_full = lax.all_gather(output_weight, "sp", axis=1, tiled=True)

    def out_term(first_row, row_span):
        row_block = lax.dynamic_slice_in_dim(attended, first_row, row_span, 0)
        return jnp.dot(row_block, out_full, preferred_element_type=jnp.float32)

    mixed = own_rows(out_term, row_count, "tp")
    return normalize(mixed, output_gain).astype(jnp.bfloat16)


MESH = pl.DeviceIdType.MESH
LANES = 128
PENALTY = 1e6


def nt_dot(left, right):
    return lax.dot_general(
        left, right, (((1,), (1,)), ((), ())), preferred_element_type=jnp.float32
    )


def nn_dot(left, right):
    return jnp.dot(left, right, preferred_element_type=jnp.float32)


def layer_kernel(
    sizes,
    tok_in,
    ids_in,
    query_down,
    latent_down,
    rope_down,
    query_up,
    key_up,
    value_up,
    out_in,
    query_gain_in,
    latent_gain_in,
    output_gain_in,
    table,
    out,
    ids,
    query_gain,
    latent_gain,
    output_gain,
    tok,
    query_down_buf,
    latent_down_buf,
    rope_down_buf,
    query_up_buf,
    key_up_buf,
    value_up_buf,
    out_w,
    table_buf,
    pack,
    query_pack,
    kv_pack,
    tok_all,
    tok_flat,
    down_all,
    query_all,
    kvup_all,
    out_all,
    raw_all,
    row_buf,
    row_all,
    part_buf,
    part_all,
    weight_send,
    weight_recv,
    row_send,
    row_recv,
    core_send,
    core_recv,
    tok_send,
    tok_recv,
    raw_send,
    raw_recv,
    part_send,
    part_recv,
    local_sem,
):
    S, T, H, N, V, R = (sizes[k] for k in ("S", "T", "H", "N", "V", "R"))
    QW, LW = sizes["QW"], sizes["LW"]
    f32, bf16 = jnp.float32, jnp.bfloat16
    rows = tok.shape[0]
    span = rows * T
    half = S // 2
    h2 = R // 2
    depth = query_down.shape[0]
    share = down_all.shape[1]
    s = lax.axis_index("sp")
    t = lax.axis_index("tp")
    pair = s + 1 - 2 * (s % 2)
    twin = t + 1 - 2 * (t % 2)

    def line(k):
        return (s + 2 * k) % S

    def mate(k):
        return (t + k) % T

    def remote(src, dst, send, recv, sp, tp):
        return pltpu.make_async_remote_copy(
            src_ref=src, dst_ref=dst, send_sem=send, recv_sem=recv,
            device_id={"sp": sp, "tp": tp}, device_id_type=MESH)

    barrier = pltpu.get_barrier_semaphore()
    for k in range(1, half):
        pl.semaphore_signal(barrier, inc=1, device_id={"sp": line(k), "tp": t}, device_id_type=MESH)
    pl.semaphore_signal(barrier, inc=1, device_id={"sp": pair, "tp": t}, device_id_type=MESH)
    for k in range(1, T):
        pl.semaphore_signal(barrier, inc=1, device_id={"sp": s, "tp": mate(k)}, device_id_type=MESH)

    loads = [
        (query_down, query_down_buf),
        (latent_down, latent_down_buf),
        (rope_down, rope_down_buf),
        (tok_in, tok),
        (query_up, query_up_buf),
        (key_up, key_up_buf),
        (value_up, value_up_buf),
        (out_in, out_w),
        (table.at[:, pl.ds(pl.multiple_of(s * span, 8), span)], table_buf),
        (ids_in, ids),
        (query_gain_in, query_gain),
        (latent_gain_in, latent_gain),
        (output_gain_in, output_gain),
    ]
    copies = []
    for i, (src, dst) in enumerate(loads):
        copy = pltpu.make_async_copy(src, dst, local_sem.at[i])
        copy.start()
        copies.append(copy)

    for copy in copies[:3]:
        copy.wait()
    pack[:QW] = query_down_buf[...].astype(f32).T.astype(bf16)
    pack[QW + LANES:] = latent_down_buf[...].astype(f32).T.astype(bf16)
    rope_cols = rope_down_buf[...].astype(f32)
    gap = jnp.zeros((LANES // 2 - h2, depth), f32)
    pack[QW:QW + LANES] = jnp.concatenate(
        [rope_cols[:h2], gap, rope_cols[h2:R], gap], axis=0).astype(bf16)
    down = pack.at[pl.ds(pl.multiple_of(t * share, 16), share)]
    copies[3].wait()
    pl.semaphore_wait(barrier, half - 1 + 1 + T - 1)

    def spread(own, view, send, recv):
        sent = []
        for k in range(1, half):
            sent.append(remote(own, view(s), send.at[k - 1], recv.at[k - 1], line(k), t))
        sent.append(remote(own, view(s), send.at[half - 1], recv.at[half - 1], pair, t))
        for copy in sent:
            copy.start()
        return sent

    def landed(view, send, recv, slot):
        remote(view(s), view(s), send.at[slot], recv.at[slot], pair, t).wait_recv()

    def pass_on(view, send, recv, sent, k):
        landed(view, send, recv, k - 1)
        block = line(half - k)
        slot = half - 1 + k
        copy = remote(view(block), view(block), send.at[slot], recv.at[slot], pair, t)
        copy.start()
        sent.append(copy)
        return block

    def pair_block(j):
        return (pair + 2 * (half - j)) % S

    def to_mates(src_of, dst, send, recv):
        sent = [remote(src_of(k), dst, send.at[k - 1], recv.at[k - 1], s, mate(k)) for k in range(1, T)]
        for copy in sent:
            copy.start()
        return sent

    wholes = [down_all, query_all, kvup_all, out_all]
    owns = [down, query_pack, kv_pack, out_w]
    views = [lambda i, w=w: w.at[i] for w in wholes]
    weight_sent = [[], [], [], []]

    def begin(i):
        weight_sent[i] += spread(owns[i], views[i], weight_send.at[i], weight_recv.at[i])

    def relay(i, then=None):
        for k in range(1, half):
            block = pass_on(views[i], weight_send.at[i], weight_recv.at[i], weight_sent[i], k)
            if then is not None:
                then(block)

    def rest(i, then=None):
        for j in range(half):
            landed(views[i], weight_send.at[i], weight_recv.at[i], half - 1 + j)
            if then is not None:
                then(pair_block(j))

    begin(0)
    tok_sent = to_mates(lambda k: tok, tok_all.at[t], tok_send, tok_recv)
    down_all[s] = down[...]
    tok_all[t] = tok[...]

    for copy in copies[4:8]:
        copy.wait()
    query_in = [query_up_buf[:, h, :].astype(f32) for h in range(H)]
    query_pack[...] = jnp.concatenate(
        [x[:, :N] for x in query_in] + [x[:, N:N + h2] for x in query_in] + [x[:, N + h2:] for x in query_in],
        axis=1).astype(bf16)
    k_rows = key_up.shape[0]
    kv_pack[:k_rows] = jnp.concatenate([key_up_buf[:, h, :].astype(f32) for h in range(H)], axis=1).astype(bf16)
    kv_pack[k_rows:] = jnp.concatenate([value_up_buf[:, h, :].astype(f32) for h in range(H)], axis=1).astype(bf16)
    query_all[s] = query_pack[...]
    kvup_all[s] = kv_pack[...]
    out_all[s] = out_w[...]

    for copy in tok_sent:
        copy.wait_recv()
    tok_flat[...] = tok_all[...].astype(f32).reshape(span, tok.shape[1]).astype(bf16)
    total_raw = [jnp.zeros((span, share), f32)]

    def down_block(block):
        columns = tok_flat[:, pl.ds(pl.multiple_of(block * depth, LANES), depth)]
        total_raw[0] = total_raw[0] + nt_dot(columns, down_all[block])

    down_block(s)
    relay(0, down_block)
    begin(1)
    begin(2)
    rest(0, down_block)
    raw_all[t] = total_raw[0].astype(bf16)
    raw_sent = to_mates(lambda k: raw_all.at[t], raw_all.at[t], raw_send, raw_recv)
    for copy in copies[8:]:
        copy.wait()
    cosine = table_buf[0]
    sine = table_buf[1]
    lane = lax.broadcasted_iota(jnp.int32, (span, LANES), 1)
    padded = -(-span // LANES) * LANES
    id_row = jnp.concatenate([ids[...].astype(f32), jnp.zeros((1, padded - span), f32)], axis=1)
    own_id = jnp.broadcast_to(id_row, (LANES, padded)).T[:span]
    id_lane = (lane - h2).astype(f32)
    is_id = (lane >= h2) & (lane < LANES // 2)

    for copy in raw_sent:
        copy.wait_recv()
    whole_raw = jnp.concatenate([raw_all[j].astype(f32) for j in range(T)], axis=1)
    query_raw = whole_raw[:, :QW]
    rope_raw = whole_raw[:, QW:QW + LANES]
    latent_raw = whole_raw[:, QW + LANES:QW + LANES + LW]

    def turn(x):
        return x * cosine + pltpu.roll(x, LANES // 2, 1) * sine

    key_marks = jnp.where(is_id & (id_lane != own_id), -1.0, 0.0)
    row_buf[:, :LW] = normalize(latent_raw, latent_gain[...][None, :]).astype(bf16)
    row_buf[:, LW:] = jnp.where(is_id, key_marks, turn(rope_raw)).astype(bf16)
    part_rows = span // 2
    mine = pl.ds(pl.multiple_of((t % 2) * part_rows, 16), part_rows)

    def row_view(i):
        return row_all.at[i, mine]

    row_sent = spread(row_buf.at[mine], row_view, row_send, row_recv)
    relay(1)
    relay(2)
    begin(3)

    query_lat = normalize(query_raw, query_gain[...][None, :]).astype(bf16)
    rest(1)
    queries = nn_dot(query_lat, query_all[...].reshape(QW, query_pack.shape[1]))
    nope = queries[:, :H * N].astype(bf16)
    rope = turn(queries[:, H * N:])
    nope_lane = lax.broadcasted_iota(jnp.int32, (span, H * N), 1)
    spread_nope = jnp.concatenate(
        [jnp.where((nope_lane >= h * N) & (nope_lane < (h + 1) * N), nope, jnp.zeros_like(nope)) for h in range(H)],
        axis=0)
    is_rope = (lane < h2) | ((lane >= LANES // 2) & (lane < LANES // 2 + h2))
    query_marks = jnp.where(is_id & (id_lane == own_id), PENALTY, 0.0)
    spread_rope = jnp.concatenate(
        [jnp.where(is_rope, rope if h == 0 else pltpu.roll(rope, LANES - h * h2, 1), query_marks).astype(bf16) for h in range(H)],
        axis=0)
    core_sent = []

    def to_twin(block, slot):
        copy = remote(row_view(block), row_view(block), core_send.at[slot], core_recv.at[slot], s, twin)
        copy.start()
        core_sent.append(copy)

    rest(2)
    key_matrix = kvup_all[:, :k_rows, :].reshape(LW, kv_pack.shape[1])
    value_matrix = kvup_all[:, k_rows:, :].reshape(LW, kv_pack.shape[1])
    absorbed = nt_dot(spread_nope, key_matrix).astype(bf16)
    wide_query = jnp.concatenate([absorbed, spread_rope], axis=1)
    scale = (N + R) ** (-0.5)

    def block_scores(key_rows):
        return nt_dot(wide_query, key_rows) * scale

    first = block_scores(row_buf[...])
    peak = jnp.max(first, axis=-1, keepdims=True)
    first = jnp.exp(first - peak)
    state = [peak, jnp.sum(first, axis=-1, keepdims=True), nn_dot(first.astype(bf16), row_buf[:, :LW])]

    def fold(blocks):
        key_rows = jnp.concatenate([row_all[b] for b in blocks], axis=0)
        scores = block_scores(key_rows)
        peak, total, running = state
        peak_new = jnp.maximum(peak, jnp.max(scores, axis=-1, keepdims=True))
        factor = jnp.exp(peak - peak_new)
        weights = jnp.exp(scores - peak_new)
        state[0] = peak_new
        state[1] = total * factor + jnp.sum(weights, axis=-1, keepdims=True)
        state[2] = running * factor + nn_dot(weights.astype(bf16), key_rows[:, :LW])

    blocks = [pass_on(row_view, row_send, row_recv, row_sent, k) for k in range(1, half)]
    for slot, block in enumerate(blocks):
        to_twin(block, slot)
    landed(row_view, row_send, row_recv, half - 1)
    to_twin(pair, half - 1)
    blocks.append(pair)
    for copy in core_sent:
        copy.wait_recv()
    relay(3)
    fold(blocks)
    for j in range(1, half):
        landed(row_view, row_send, row_recv, half - 1 + j)
        to_twin(pair_block(j), half - 1 + j)
    for copy in core_sent[half:]:
        copy.wait_recv()
    fold([pair_block(j) for j in range(1, half)])
    averaged = state[2] / state[1]
    everything = nn_dot(averaged.astype(bf16), value_matrix)
    value_lane = lax.broadcasted_iota(jnp.int32, (span, H * V), 1)
    attended = jnp.zeros((span, H * V), f32)
    for h in range(H):
        attended = jnp.where(
            (value_lane >= h * V) & (value_lane < (h + 1) * V), everything[h * span:(h + 1) * span], attended)
    attended = attended.astype(bf16)
    columns = out_w.shape[1]
    part_sent = []

    def project(side):
        for j in range(half):
            part = nn_dot(attended, out_all[2 * j + side])
            for i in range(T):
                part_buf[i, side, :, j * columns:(j + 1) * columns] = part[i * rows:(i + 1) * rows].astype(bf16)
        group = []
        for k in range(1, T):
            n = len(part_sent) * (T - 1) + k - 1
            group.append(remote(
                part_buf.at[mate(k), side], part_all.at[k - 1, side], part_send.at[n], part_recv.at[n], s, mate(k)))
            group[-1].start()
        part_sent.append(group)

    project(s % 2)
    rest(3)
    project(1 - s % 2)
    for group in part_sent:
        for copy in group:
            copy.wait_recv()
    sides = []
    for side in range(2):
        total = part_buf[t, side].astype(f32)
        for k in range(1, T):
            total = total + part_all[k - 1, side].astype(f32)
        sides.append(total)
    mixed = jnp.concatenate(
        [sides[j % 2][:, (j // 2) * columns:(j // 2 + 1) * columns] for j in range(S)], axis=1)
    out[...] = normalize(mixed, output_gain[...][None, :]).astype(bf16)
    for copy in tok_sent + raw_sent + row_sent + core_sent + [c for group in part_sent for c in group] + [c for group in weight_sent for c in group]:
        copy.wait_send()


def kernel_fits(mesh, tokens, query_down, query_up, latent_down, rope_down, key_up, value_up, output_weight):
    S, T = mesh.shape["sp"], mesh.shape["tp"]
    H, N, V, R = query_up.shape[1], key_up.shape[2], value_up.shape[2], rope_down.shape[1]
    columns = query_down.shape[1] + latent_down.shape[1] + LANES
    return (
        S % 2 == 0 and S >= 4
        and tokens.shape[0] % 8 == 0
        and query_down.shape[0] % LANES == 0
        and query_down.shape[1] % LANES == 0
        and latent_down.shape[1] % LANES == 0
        and columns % (16 * T) == 0
        and query_up.shape[0] % 16 == 0
        and key_up.shape[0] % 16 == 0
        and output_weight.shape[1] % LANES == 0
        and H * R == LANES
        and T % 2 == 0
        and (tokens.shape[0] * T) % 32 == 0
        and R % 32 == 0
        and query_down.shape[0] == LANES
        and H * N % LANES == 0
        and N == V
    )


def rope_tables(positions, width, copies):
    h2 = width // 2
    frequency = ROPE_BASE ** (-np.arange(0, width, 2, dtype=np.float64) / width)
    angles = np.arange(positions, dtype=np.float64)[:, None] * frequency[None, :]
    cosine = np.tile(np.cos(angles), (1, 2 * copies))
    sine = np.tile(np.sin(angles), (1, copies))
    return np.stack([cosine, np.concatenate([-sine, sine], axis=1)]).astype(np.float32)


def on_device(mesh, tokens, doc_ids, query_down, query_gain, query_up, latent_down, latent_gain,
              rope_down, key_up, value_up, output_weight, output_gain):
    if not kernel_fits(mesh, tokens, query_down, query_up, latent_down, rope_down, key_up, value_up, output_weight):
        return plain_layer(tokens, doc_ids, query_down, query_gain, query_up, latent_down, latent_gain,
                           rope_down, key_up, value_up, output_weight, output_gain)
    S, T = mesh.shape["sp"], mesh.shape["tp"]
    H, N, V, R = query_up.shape[1], key_up.shape[2], value_up.shape[2], rope_down.shape[1]
    QW, LW = query_down.shape[1], latent_down.shape[1]
    rows, width = tokens.shape
    span = rows * T
    share = (QW + LANES + LW) // T
    table = jnp.asarray(rope_tables(S * span, R, H))
    sizes = dict(S=S, T=T, H=H, N=N, V=V, R=R, QW=QW, LW=LW)
    vmem = pl.BlockSpec(memory_space=pltpu.VMEM)
    bf16 = jnp.bfloat16
    sem = pltpu.SemaphoreType.DMA
    hbm = pl.BlockSpec(memory_space=pltpu.HBM)
    wq = (query_up.shape[0], H * (N + R))
    wkv = (2 * key_up.shape[0], H * N)
    return pl.pallas_call(
        functools.partial(layer_kernel, sizes),
        out_shape=jax.ShapeDtypeStruct((rows, width), bf16),
        in_specs=[hbm] * 13,
        out_specs=vmem,
        scratch_shapes=[
            pltpu.VMEM((1, span), jnp.int32),
            pltpu.VMEM((QW,), jnp.float32),
            pltpu.VMEM((LW,), jnp.float32),
            pltpu.VMEM((width,), jnp.float32),
            pltpu.VMEM(tokens.shape, bf16),
            pltpu.VMEM(query_down.shape, bf16),
            pltpu.VMEM(latent_down.shape, bf16),
            pltpu.VMEM(rope_down.shape[::-1], bf16),
            pltpu.VMEM(query_up.shape, bf16),
            pltpu.VMEM(key_up.shape, bf16),
            pltpu.VMEM(value_up.shape, bf16),
            pltpu.VMEM(output_weight.shape, bf16),
            pltpu.VMEM((2, span, LANES), jnp.float32),
            pltpu.VMEM((QW + LANES + LW, query_down.shape[0]), bf16),
            pltpu.VMEM(wq, bf16),
            pltpu.VMEM(wkv, bf16),
            pltpu.VMEM((T, rows, width), bf16),
            pltpu.VMEM((span, width), bf16),
            pltpu.VMEM((S, share, query_down.shape[0]), bf16),
            pltpu.VMEM((S,) + wq, bf16),
            pltpu.VMEM((S,) + wkv, bf16),
            pltpu.VMEM((S,) + output_weight.shape, bf16),
            pltpu.VMEM((T, span, share), bf16),
            pltpu.VMEM((span, LW + LANES), bf16),
            pltpu.VMEM((S, span, LW + LANES), bf16),
            pltpu.VMEM((T, 2, rows, width // 2), bf16),
            pltpu.VMEM((T - 1, 2, rows, width // 2), bf16),
            sem((4, S - 1)),
            sem((4, S - 1)),
            sem((S - 1,)),
            sem((S - 1,)),
            sem((S - 1,)),
            sem((S - 1,)),
            sem((T - 1,)),
            sem((T - 1,)),
            sem((T - 1,)),
            sem((T - 1,)),
            sem((2 * (T - 1),)),
            sem((2 * (T - 1),)),
            sem((13,)),
        ],
        compiler_params=pltpu.CompilerParams(
            collective_id=0, has_side_effects=True, vmem_limit_bytes=67043328),
    )(tokens, doc_ids[None, :], query_down, latent_down, rope_down.T, query_up, key_up, value_up, output_weight,
      query_gain, latent_gain, output_gain, table)


def solution(mesh):
    in_specs = (
        P(("sp", "tp"), None),
        P("sp"),
        P("sp", None),
        P(),
        P("sp", "tp", None),
        P("sp", None),
        P(),
        P("sp", None),
        P("sp", "tp", None),
        P("sp", "tp", None),
        P("tp", "sp"),
        P(),
    )
    out_specs = P(("sp", "tp"), None)
    return jax.shard_map(
        functools.partial(on_device, mesh), mesh=mesh, in_specs=in_specs, out_specs=out_specs, check_vma=False
    )
```

```python
import functools

import jax
import jax.numpy as jnp
import numpy as np
from jax import lax
from jax.experimental import pallas as pl
from jax.experimental.pallas import tpu as pltpu
from jax.sharding import PartitionSpec as P

ROPE_BASE = 10000.0
EPS = 1e-06
MASKED = -1e30


def folded(value, axis, dim, update, carry):
    whole = jax.tree.map(lambda part: lax.all_gather(part, axis, axis=dim, tiled=True), value)
    return update(carry, whole, jnp.int32(0))


def gathered_then(share, axis, dim, apply):
    everything = lax.all_gather(share, axis, axis=dim, tiled=True)
    return apply(everything, jnp.int32(0))


def for_sending(value):
    def short(part):
        return part.astype(jnp.bfloat16) if part.dtype == jnp.float32 else part

    return jax.tree.map(short, value)


def own_rows(term, extent, axis):
    whole = term(jnp.int32(0), extent * lax.axis_size(axis)).astype(jnp.bfloat16)
    return lax.psum_scatter(whole, axis, scatter_dimension=0, tiled=True).astype(jnp.float32)


def normalize(values, gain_vec):
    return values * lax.rsqrt(jnp.mean(values * values, axis=-1, keepdims=True) + EPS) * gain_vec


def rotate(rope_part, position):
    half_width = rope_part.shape[-1] // 2
    frequency = ROPE_BASE ** (
        -jnp.arange(0, 2 * half_width, 2, dtype=jnp.float32) / (2 * half_width)
    )
    angles = position.astype(jnp.float32)[:, None] * frequency[None, :]
    cosine = jnp.cos(angles)
    sine_part = jnp.sin(angles)
    if rope_part.ndim == 3:
        cosine = cosine[:, None, :]
        sine_part = sine_part[:, None, :]
    first_half = rope_part[..., :half_width]
    second_half = rope_part[..., half_width:]
    return jnp.concatenate(
        [
            first_half * cosine - second_half * sine_part,
            first_half * sine_part + second_half * cosine,
        ],
        axis=-1,
    )


def plain_layer(
    tokens,
    doc_ids,
    query_down,
    query_gain,
    query_up,
    latent_down,
    latent_gain,
    rope_down,
    key_up,
    value_up,
    output_weight,
    output_gain,
):
    row_count = tokens.shape[0]
    key_span = doc_ids.shape[0]
    query_width = query_down.shape[1]
    latent_width = latent_down.shape[1]
    rope_width = rope_down.shape[1]
    local_heads = query_up.shape[1]
    head_width = query_up.shape[2]
    nope_width = key_up.shape[2]
    value_width = value_up.shape[2]

    def down_term(total_now, weight_rows, first_row):
        columns = lax.dynamic_slice_in_dim(tokens, first_row, weight_rows.shape[0], 1)
        return total_now + jnp.dot(columns, weight_rows, preferred_element_type=jnp.float32)

    empty_query = jnp.zeros((row_count, query_width), jnp.float32)
    empty_latent = jnp.zeros((row_count, latent_width), jnp.float32)
    empty_rope = jnp.zeros((row_count, rope_width), jnp.float32)
    query_sum = folded(query_down, "sp", 0, down_term, empty_query)
    latent_sum = folded(latent_down, "sp", 0, down_term, empty_latent)
    rope_sum = folded(rope_down, "sp", 0, down_term, empty_rope)
    query_lat = normalize(query_sum, query_gain).astype(jnp.bfloat16)
    kv_lat = normalize(latent_sum, latent_gain).astype(jnp.bfloat16)
    own_position = lax.axis_index(("sp", "tp")) * row_count + lax.iota(jnp.int32, row_count)
    rope_keys = rotate(rope_sum, own_position).astype(jnp.bfloat16)
    query_full, key_full, value_full = (
        lax.all_gather(query_up, "sp", axis=0, tiled=True),
        lax.all_gather(key_up, "sp", axis=0, tiled=True),
        lax.all_gather(value_up, "sp", axis=0, tiled=True),
    )
    flat_width = local_heads * head_width
    query_matrix = query_full.reshape(query_width, flat_width)
    block_offset = lax.axis_index("sp") * key_span

    def project(latent_rows, first_row):
        piece_rows = latent_rows.shape[0]
        raw_query = jnp.dot(
            latent_rows[:, :query_width], query_matrix, preferred_element_type=jnp.float32
        ).reshape(piece_rows, local_heads, head_width)
        position = block_offset + first_row + lax.iota(jnp.int32, piece_rows)
        turned = jnp.concatenate(
            [raw_query[..., :nope_width], rotate(raw_query[..., nope_width:], position)], axis=-1
        )
        return jnp.concatenate(
            [
                turned.astype(jnp.bfloat16).reshape(piece_rows, flat_width),
                latent_rows[:, query_width:],
            ],
            axis=1,
        )

    packed = jnp.concatenate([query_lat, kv_lat, rope_keys], axis=1)
    gathered = gathered_then(packed, "tp", 0, project)
    queries = gathered[:, :flat_width].reshape(key_span, local_heads, head_width)
    my_ids = doc_ids.astype(jnp.bfloat16)
    key_rows = jnp.concatenate([gathered[:, flat_width:], my_ids[:, None]], axis=1)
    query_nope = queries[..., :nope_width]
    query_rope = queries[..., nope_width:]
    score_scale = head_width ** (-0.5)
    absorbed = jnp.einsum("qhe,rhe->qhr", query_nope, key_full, preferred_element_type=jnp.float32)

    def block_scores(latent_part, rope_part):
        latent_float = latent_part.astype(jnp.float32)
        scores = jnp.einsum("qhr,kr->qhk", absorbed, latent_float, precision=lax.Precision.HIGHEST)
        scores = scores + jnp.einsum(
            "qhe,ke->qhk", query_rope, rope_part, preferred_element_type=jnp.float32
        )
        return (scores * score_scale, latent_float)

    def finish(averaged):
        return jnp.einsum(
            "qhr,rhv->qhv",
            averaged,
            value_full.astype(jnp.float32),
            precision=lax.Precision.HIGHEST,
        )

    def scan_step(state_now, block_keys):
        row_peak, row_total, running = state_now
        latent_part = block_keys[:, :latent_width]
        rope_part = block_keys[:, latent_width : latent_width + rope_width]
        block_ids = block_keys[:, latent_width + rope_width]
        scores, value_part = block_scores(latent_part, rope_part)
        same_doc = my_ids[:, None, None] == block_ids[None, None, :]
        peak_new = jnp.maximum(row_peak, jnp.max(jnp.where(same_doc, scores, MASKED), axis=-1))
        soft_weights = jnp.where(same_doc, jnp.exp(scores - peak_new[..., None]), 0.0)
        factor = jnp.exp(row_peak - peak_new)
        if value_part.ndim == 3:
            contrib = jnp.einsum(
                "qhk,khv->qhv", soft_weights, value_part, precision=lax.Precision.HIGHEST
            )
        else:
            contrib = jnp.einsum(
                "qhk,kv->qhv", soft_weights, value_part, precision=lax.Precision.HIGHEST
            )
        next_state = (
            peak_new,
            row_total * factor + jnp.sum(soft_weights, axis=-1),
            running * factor[..., None] + contrib,
        )
        return (next_state, None)

    def fold_keys(state_now, key_piece, first_row):
        key_blocks = key_piece.reshape(key_piece.shape[0] // key_span, key_span, key_piece.shape[1])
        return lax.scan(scan_step, state_now, key_blocks)[0]

    start_state = (
        jnp.full((key_span, local_heads), MASKED, jnp.float32),
        jnp.zeros((key_span, local_heads), jnp.float32),
        jnp.zeros((key_span, local_heads, latent_width), jnp.float32),
    )
    row_peak, row_total, running = folded(for_sending(key_rows), "sp", 0, fold_keys, start_state)
    averaged = running / row_total[..., None]
    attended = finish(averaged).astype(jnp.bfloat16).reshape(key_span, local_heads * value_width)
    out_full = lax.all_gather(output_weight, "sp", axis=1, tiled=True)

    def out_term(first_row, row_span):
        row_block = lax.dynamic_slice_in_dim(attended, first_row, row_span, 0)
        return jnp.dot(row_block, out_full, preferred_element_type=jnp.float32)

    mixed = own_rows(out_term, row_count, "tp")
    return normalize(mixed, output_gain).astype(jnp.bfloat16)


MESH = pl.DeviceIdType.MESH
LANES = 128
PENALTY = 1e6


def nt_dot(left, right):
    return lax.dot_general(
        left, right, (((1,), (1,)), ((), ())), preferred_element_type=jnp.float32
    )


def nn_dot(left, right):
    return jnp.dot(left, right, preferred_element_type=jnp.float32)


def layer_kernel(
    sizes,
    tok_in,
    ids_in,
    query_down,
    latent_down,
    rope_down,
    query_up,
    key_up,
    value_up,
    out_in,
    query_gain_in,
    latent_gain_in,
    output_gain_in,
    table,
    out,
    ids,
    query_gain,
    latent_gain,
    output_gain,
    tok,
    query_down_buf,
    latent_down_buf,
    rope_down_buf,
    query_up_buf,
    key_up_buf,
    value_up_buf,
    out_w,
    table_buf,
    pack,
    query_pack,
    kv_pack,
    tok_all,
    tok_flat,
    down_all,
    query_all,
    kvup_all,
    out_all,
    raw_all,
    row_buf,
    row_all,
    part_buf,
    part_all,
    weight_send,
    weight_recv,
    row_send,
    row_recv,
    core_send,
    core_recv,
    tok_send,
    tok_recv,
    raw_send,
    raw_recv,
    part_send,
    part_recv,
    local_sem,
):
    S, T, H, N, V, R = (sizes[k] for k in ("S", "T", "H", "N", "V", "R"))
    QW, LW = sizes["QW"], sizes["LW"]
    f32, bf16 = jnp.float32, jnp.bfloat16
    rows = tok.shape[0]
    span = rows * T
    half = S // 2
    h2 = R // 2
    depth = query_down.shape[0]
    share = down_all.shape[1]
    s = lax.axis_index("sp")
    t = lax.axis_index("tp")
    pair = s + 1 - 2 * (s % 2)
    twin = t + 1 - 2 * (t % 2)

    def line(k):
        return (s + 2 * k) % S

    def mate(k):
        return (t + k) % T

    def remote(src, dst, send, recv, sp, tp):
        return pltpu.make_async_remote_copy(
            src_ref=src, dst_ref=dst, send_sem=send, recv_sem=recv,
            device_id={"sp": sp, "tp": tp}, device_id_type=MESH)

    barrier = pltpu.get_barrier_semaphore()
    for k in range(1, half):
        pl.semaphore_signal(barrier, inc=1, device_id={"sp": line(k), "tp": t}, device_id_type=MESH)
    pl.semaphore_signal(barrier, inc=1, device_id={"sp": pair, "tp": t}, device_id_type=MESH)
    for k in range(1, T):
        pl.semaphore_signal(barrier, inc=1, device_id={"sp": s, "tp": mate(k)}, device_id_type=MESH)

    loads = [
        (query_down, query_down_buf),
        (latent_down, latent_down_buf),
        (rope_down, rope_down_buf),
        (tok_in, tok),
        (query_up, query_up_buf),
        (key_up, key_up_buf),
        (value_up, value_up_buf),
        (out_in, out_w),
        (table.at[:, pl.ds(pl.multiple_of(s * span, 8), span)], table_buf),
        (ids_in, ids),
        (query_gain_in, query_gain),
        (latent_gain_in, latent_gain),
        (output_gain_in, output_gain),
    ]
    copies = []
    for i, (src, dst) in enumerate(loads):
        copy = pltpu.make_async_copy(src, dst, local_sem.at[i])
        copy.start()
        copies.append(copy)

    for copy in copies[:3]:
        copy.wait()
    pack[:QW] = query_down_buf[...].astype(f32).T.astype(bf16)
    pack[QW + LANES:] = latent_down_buf[...].astype(f32).T.astype(bf16)
    rope_cols = rope_down_buf[...].astype(f32)
    gap = jnp.zeros((LANES // 2 - h2, depth), f32)
    pack[QW:QW + LANES] = jnp.concatenate(
        [rope_cols[:h2], gap, rope_cols[h2:R], gap], axis=0).astype(bf16)
    down = pack.at[pl.ds(pl.multiple_of(t * share, 16), share)]
    copies[3].wait()
    pl.semaphore_wait(barrier, half - 1 + 1 + T - 1)

    def spread(own, view, send, recv):
        sent = []
        for k in range(1, half):
            sent.append(remote(own, view(s), send.at[k - 1], recv.at[k - 1], line(k), t))
        sent.append(remote(own, view(s), send.at[half - 1], recv.at[half - 1], pair, t))
        for copy in sent:
            copy.start()
        return sent

    def landed(view, send, recv, slot):
        remote(view(s), view(s), send.at[slot], recv.at[slot], pair, t).wait_recv()

    def pass_on(view, send, recv, sent, k):
        landed(view, send, recv, k - 1)
        block = line(half - k)
        slot = half - 1 + k
        copy = remote(view(block), view(block), send.at[slot], recv.at[slot], pair, t)
        copy.start()
        sent.append(copy)
        return block

    def pair_block(j):
        return (pair + 2 * (half - j)) % S

    def to_mates(src_of, dst, send, recv):
        sent = [remote(src_of(k), dst, send.at[k - 1], recv.at[k - 1], s, mate(k)) for k in range(1, T)]
        for copy in sent:
            copy.start()
        return sent

    wholes = [down_all, query_all, kvup_all, out_all]
    owns = [down, query_pack, kv_pack, out_w]
    views = [lambda i, w=w: w.at[i] for w in wholes]
    weight_sent = [[], [], [], []]

    def begin(i):
        weight_sent[i] += spread(owns[i], views[i], weight_send.at[i], weight_recv.at[i])

    def relay(i, then=None):
        for k in range(1, half):
            block = pass_on(views[i], weight_send.at[i], weight_recv.at[i], weight_sent[i], k)
            if then is not None:
                then(block)

    def rest(i, then=None):
        for j in range(half):
            landed(views[i], weight_send.at[i], weight_recv.at[i], half - 1 + j)
            if then is not None:
                then(pair_block(j))

    begin(0)
    tok_sent = to_mates(lambda k: tok, tok_all.at[t], tok_send, tok_recv)
    down_all[s] = down[...]
    tok_all[t] = tok[...]

    for copy in copies[4:8]:
        copy.wait()
    query_in = [query_up_buf[:, h, :].astype(f32) for h in range(H)]
    query_pack[...] = jnp.concatenate(
        [x[:, :N] for x in query_in] + [x[:, N:N + h2] for x in query_in] + [x[:, N + h2:] for x in query_in],
        axis=1).astype(bf16)
    k_rows = key_up.shape[0]
    kv_pack[:k_rows] = jnp.concatenate([key_up_buf[:, h, :].astype(f32) for h in range(H)], axis=1).astype(bf16)
    kv_pack[k_rows:] = jnp.concatenate([value_up_buf[:, h, :].astype(f32) for h in range(H)], axis=1).astype(bf16)
    query_all[s] = query_pack[...]
    kvup_all[s] = kv_pack[...]
    out_all[s] = out_w[...]

    for copy in tok_sent:
        copy.wait_recv()
    tok_flat[...] = tok_all[...].astype(f32).reshape(span, tok.shape[1]).astype(bf16)
    total_raw = [jnp.zeros((span, share), f32)]

    def down_block(block):
        columns = tok_flat[:, pl.ds(pl.multiple_of(block * depth, LANES), depth)]
        total_raw[0] = total_raw[0] + nt_dot(columns, down_all[block])

    down_block(s)
    relay(0, down_block)
    begin(1)
    begin(2)
    rest(0, down_block)
    raw_all[t] = total_raw[0].astype(bf16)
    raw_sent = to_mates(lambda k: raw_all.at[t], raw_all.at[t], raw_send, raw_recv)
    for copy in copies[8:]:
        copy.wait()
    cosine = table_buf[0]
    sine = table_buf[1]
    lane = lax.broadcasted_iota(jnp.int32, (span, LANES), 1)
    padded = -(-span // LANES) * LANES
    id_row = jnp.concatenate([ids[...].astype(f32), jnp.zeros((1, padded - span), f32)], axis=1)
    own_id = jnp.broadcast_to(id_row, (LANES, padded)).T[:span]
    id_lane = (lane - h2).astype(f32)
    is_id = (lane >= h2) & (lane < LANES // 2)

    relay(1)
    relay(2)
    for copy in raw_sent:
        copy.wait_recv()
    whole_raw = jnp.concatenate([raw_all[j].astype(f32) for j in range(T)], axis=1)
    query_raw = whole_raw[:, :QW]
    rope_raw = whole_raw[:, QW:QW + LANES]
    latent_raw = whole_raw[:, QW + LANES:QW + LANES + LW]

    def turn(x):
        return x * cosine + pltpu.roll(x, LANES // 2, 1) * sine

    key_marks = jnp.where(is_id & (id_lane != own_id), -1.0, 0.0)
    row_buf[:, :LW] = normalize(latent_raw, latent_gain[...][None, :]).astype(bf16)
    row_buf[:, LW:] = jnp.where(is_id, key_marks, turn(rope_raw)).astype(bf16)
    part_rows = span // 2
    mine = pl.ds(pl.multiple_of((t % 2) * part_rows, 16), part_rows)

    def row_view(i):
        return row_all.at[i, mine]

    row_sent = spread(row_buf.at[mine], row_view, row_send, row_recv)
    begin(3)

    query_lat = normalize(query_raw, query_gain[...][None, :]).astype(bf16)
    rest(1)
    queries = nn_dot(query_lat, query_all[...].reshape(QW, query_pack.shape[1]))
    nope = queries[:, :H * N].astype(bf16)
    rope = turn(queries[:, H * N:])
    nope_lane = lax.broadcasted_iota(jnp.int32, (span, H * N), 1)
    spread_nope = jnp.concatenate(
        [jnp.where((nope_lane >= h * N) & (nope_lane < (h + 1) * N), nope, jnp.zeros_like(nope)) for h in range(H)],
        axis=0)
    is_rope = (lane < h2) | ((lane >= LANES // 2) & (lane < LANES // 2 + h2))
    query_marks = jnp.where(is_id & (id_lane == own_id), PENALTY, 0.0)
    spread_rope = jnp.concatenate(
        [jnp.where(is_rope, rope if h == 0 else pltpu.roll(rope, LANES - h * h2, 1), query_marks).astype(bf16) for h in range(H)],
        axis=0)
    core_sent = []

    def to_twin(block, slot):
        copy = remote(row_view(block), row_view(block), core_send.at[slot], core_recv.at[slot], s, twin)
        copy.start()
        core_sent.append(copy)

    rest(2)
    key_matrix = kvup_all[:, :k_rows, :].reshape(LW, kv_pack.shape[1])
    value_matrix = kvup_all[:, k_rows:, :].reshape(LW, kv_pack.shape[1])
    absorbed = nt_dot(spread_nope, key_matrix).astype(bf16)
    wide_query = jnp.concatenate([absorbed, spread_rope], axis=1)
    scale = (N + R) ** (-0.5)

    def block_scores(key_rows):
        return nt_dot(wide_query, key_rows) * scale

    first = block_scores(row_buf[...])
    peak = jnp.max(first, axis=-1, keepdims=True)
    first = jnp.exp(first - peak)
    state = [peak, jnp.sum(first, axis=-1, keepdims=True), nn_dot(first.astype(bf16), row_buf[:, :LW])]

    def fold(blocks):
        key_rows = jnp.concatenate([row_all[b] for b in blocks], axis=0)
        scores = block_scores(key_rows)
        peak, total, running = state
        peak_new = jnp.maximum(peak, jnp.max(scores, axis=-1, keepdims=True))
        factor = jnp.exp(peak - peak_new)
        weights = jnp.exp(scores - peak_new)
        state[0] = peak_new
        state[1] = total * factor + jnp.sum(weights, axis=-1, keepdims=True)
        state[2] = running * factor + nn_dot(weights.astype(bf16), key_rows[:, :LW])

    blocks = [pass_on(row_view, row_send, row_recv, row_sent, k) for k in range(1, half)]
    for slot, block in enumerate(blocks):
        to_twin(block, slot)
    landed(row_view, row_send, row_recv, half - 1)
    to_twin(pair, half - 1)
    blocks.append(pair)
    for copy in core_sent:
        copy.wait_recv()
    relay(3)
    fold(blocks)
    for j in range(1, half):
        landed(row_view, row_send, row_recv, half - 1 + j)
        to_twin(pair_block(j), half - 1 + j)
    for copy in core_sent[half:]:
        copy.wait_recv()
    fold([pair_block(j) for j in range(1, half)])
    averaged = state[2] / state[1]
    everything = nn_dot(averaged.astype(bf16), value_matrix)
    value_lane = lax.broadcasted_iota(jnp.int32, (span, H * V), 1)
    attended = jnp.zeros((span, H * V), f32)
    for h in range(H):
        attended = jnp.where(
            (value_lane >= h * V) & (value_lane < (h + 1) * V), everything[h * span:(h + 1) * span], attended)
    attended = attended.astype(bf16)
    columns = out_w.shape[1]
    part_sent = []

    def project(side):
        for j in range(half):
            part = nn_dot(attended, out_all[2 * j + side])
            for i in range(T):
                part_buf[i, side, :, j * columns:(j + 1) * columns] = part[i * rows:(i + 1) * rows].astype(bf16)
        group = []
        for k in range(1, T):
            n = len(part_sent) * (T - 1) + k - 1
            group.append(remote(
                part_buf.at[mate(k), side], part_all.at[k - 1, side], part_send.at[n], part_recv.at[n], s, mate(k)))
            group[-1].start()
        part_sent.append(group)

    project(s % 2)
    rest(3)
    project(1 - s % 2)
    for group in part_sent:
        for copy in group:
            copy.wait_recv()
    sides = []
    for side in range(2):
        total = part_buf[t, side].astype(f32)
        for k in range(1, T):
            total = total + part_all[k - 1, side].astype(f32)
        sides.append(total)
    mixed = jnp.concatenate(
        [sides[j % 2][:, (j // 2) * columns:(j // 2 + 1) * columns] for j in range(S)], axis=1)
    out[...] = normalize(mixed, output_gain[...][None, :]).astype(bf16)
    for copy in tok_sent + raw_sent + row_sent + core_sent + [c for group in part_sent for c in group] + [c for group in weight_sent for c in group]:
        copy.wait_send()


def kernel_fits(mesh, tokens, query_down, query_up, latent_down, rope_down, key_up, value_up, output_weight):
    S, T = mesh.shape["sp"], mesh.shape["tp"]
    H, N, V, R = query_up.shape[1], key_up.shape[2], value_up.shape[2], rope_down.shape[1]
    columns = query_down.shape[1] + latent_down.shape[1] + LANES
    return (
        S % 2 == 0 and S >= 4
        and tokens.shape[0] % 8 == 0
        and query_down.shape[0] % LANES == 0
        and query_down.shape[1] % LANES == 0
        and latent_down.shape[1] % LANES == 0
        and columns % (16 * T) == 0
        and query_up.shape[0] % 16 == 0
        and key_up.shape[0] % 16 == 0
        and output_weight.shape[1] % LANES == 0
        and H * R == LANES
        and T % 2 == 0
        and (tokens.shape[0] * T) % 32 == 0
        and R % 32 == 0
        and query_down.shape[0] == LANES
        and H * N % LANES == 0
        and N == V
    )


def rope_tables(positions, width, copies):
    h2 = width // 2
    frequency = ROPE_BASE ** (-np.arange(0, width, 2, dtype=np.float64) / width)
    angles = np.arange(positions, dtype=np.float64)[:, None] * frequency[None, :]
    cosine = np.tile(np.cos(angles), (1, 2 * copies))
    sine = np.tile(np.sin(angles), (1, copies))
    return np.stack([cosine, np.concatenate([-sine, sine], axis=1)]).astype(np.float32)


def on_device(mesh, tokens, doc_ids, query_down, query_gain, query_up, latent_down, latent_gain,
              rope_down, key_up, value_up, output_weight, output_gain):
    if not kernel_fits(mesh, tokens, query_down, query_up, latent_down, rope_down, key_up, value_up, output_weight):
        return plain_layer(tokens, doc_ids, query_down, query_gain, query_up, latent_down, latent_gain,
                           rope_down, key_up, value_up, output_weight, output_gain)
    S, T = mesh.shape["sp"], mesh.shape["tp"]
    H, N, V, R = query_up.shape[1], key_up.shape[2], value_up.shape[2], rope_down.shape[1]
    QW, LW = query_down.shape[1], latent_down.shape[1]
    rows, width = tokens.shape
    span = rows * T
    share = (QW + LANES + LW) // T
    table = jnp.asarray(rope_tables(S * span, R, H))
    sizes = dict(S=S, T=T, H=H, N=N, V=V, R=R, QW=QW, LW=LW)
    vmem = pl.BlockSpec(memory_space=pltpu.VMEM)
    bf16 = jnp.bfloat16
    sem = pltpu.SemaphoreType.DMA
    hbm = pl.BlockSpec(memory_space=pltpu.HBM)
    wq = (query_up.shape[0], H * (N + R))
    wkv = (2 * key_up.shape[0], H * N)
    return pl.pallas_call(
        functools.partial(layer_kernel, sizes),
        out_shape=jax.ShapeDtypeStruct((rows, width), bf16),
        in_specs=[hbm] * 13,
        out_specs=vmem,
        scratch_shapes=[
            pltpu.VMEM((1, span), jnp.int32),
            pltpu.VMEM((QW,), jnp.float32),
            pltpu.VMEM((LW,), jnp.float32),
            pltpu.VMEM((width,), jnp.float32),
            pltpu.VMEM(tokens.shape, bf16),
            pltpu.VMEM(query_down.shape, bf16),
            pltpu.VMEM(latent_down.shape, bf16),
            pltpu.VMEM(rope_down.shape[::-1], bf16),
            pltpu.VMEM(query_up.shape, bf16),
            pltpu.VMEM(key_up.shape, bf16),
            pltpu.VMEM(value_up.shape, bf16),
            pltpu.VMEM(output_weight.shape, bf16),
            pltpu.VMEM((2, span, LANES), jnp.float32),
            pltpu.VMEM((QW + LANES + LW, query_down.shape[0]), bf16),
            pltpu.VMEM(wq, bf16),
            pltpu.VMEM(wkv, bf16),
            pltpu.VMEM((T, rows, width), bf16),
            pltpu.VMEM((span, width), bf16),
            pltpu.VMEM((S, share, query_down.shape[0]), bf16),
            pltpu.VMEM((S,) + wq, bf16),
            pltpu.VMEM((S,) + wkv, bf16),
            pltpu.VMEM((S,) + output_weight.shape, bf16),
            pltpu.VMEM((T, span, share), bf16),
            pltpu.VMEM((span, LW + LANES), bf16),
            pltpu.VMEM((S, span, LW + LANES), bf16),
            pltpu.VMEM((T, 2, rows, width // 2), bf16),
            pltpu.VMEM((T - 1, 2, rows, width // 2), bf16),
            sem((4, S - 1)),
            sem((4, S - 1)),
            sem((S - 1,)),
            sem((S - 1,)),
            sem((S - 1,)),
            sem((S - 1,)),
            sem((T - 1,)),
            sem((T - 1,)),
            sem((T - 1,)),
            sem((T - 1,)),
            sem((2 * (T - 1),)),
            sem((2 * (T - 1),)),
            sem((13,)),
        ],
        compiler_params=pltpu.CompilerParams(
            collective_id=0, has_side_effects=True, vmem_limit_bytes=67043328),
    )(tokens, doc_ids[None, :], query_down, latent_down, rope_down.T, query_up, key_up, value_up, output_weight,
      query_gain, latent_gain, output_gain, table)


def solution(mesh):
    in_specs = (
        P(("sp", "tp"), None),
        P("sp"),
        P("sp", None),
        P(),
        P("sp", "tp", None),
        P("sp", None),
        P(),
        P("sp", None),
        P("sp", "tp", None),
        P("sp", "tp", None),
        P("tp", "sp"),
        P(),
    )
    out_specs = P(("sp", "tp"), None)
    return jax.shard_map(
        functools.partial(on_device, mesh), mesh=mesh, in_specs=in_specs, out_specs=out_specs, check_vma=False
    )
```
